256 devices in a mesh: grp: 4 (over y, x), ep: 64 (over z, core).
Axes of the slice: x: 2, y: 2, z: 32, core: 2. Of those that a mesh axis runs over, the one named last changes fastest.
The devices are a block of a 4x8x32 slice.
Arguments:
- tokens: bfloat16 [32768, 2048], P(('grp', 'ep')), parts along dimension 0, may hold values from -6 to 6
- norm_gain: float32 [2048], replicated, may hold values from 0.1 to 1.9
- expert_ids: int32 [32768, 2], P(('grp', 'ep')), parts along dimension 0, may hold values from 0 to 15, all different within a row; in each aligned block of 128 rows (0 to 127, 128 to 255, ...) at most 32 rows name the same one
- route_weight: float32 [32768, 2], P(('grp', 'ep')), parts along dimension 0, may hold values from 0.1 to 1
- gate_weight: bfloat16 [64, 2048, 512], P('ep'), may hold values from -0.375 to 0.375
- up_weight: bfloat16 [64, 2048, 512], P('ep'), may hold values from -0.375 to 0.375
- down_weight: bfloat16 [64, 512, 2048], P('ep'), may hold values from -0.03125 to 0.03125
Outputs:
- combined: bfloat16 [32768, 2048], P(('grp', 'ep')), parts along dimension 0
The draws below stay inside these ranges and needn't reach their ends.
There are 4 independent parts, one for each index of `grp`. The reference program is written for one: setup_inputs(seed, part) draws one part's arguments, and reference() takes and returns one part's arrays. A program takes and returns all parts, laid end to end along the dimension named above; an argument that names none is the same for every part. Nothing has to cross between parts.
Inputs may be any that keep to these rules, and one draw needn't show every extreme that they name: `expert_ids`: each token names 2 different experts; among the tokens of one device no expert is named more than 32 times, and in every draw some expert is named exactly 32 times by the tokens of some device.
All inputs are finite; a program needn't handle non-finite values.
Results may differ from the reference program's by a relative error of at most 0.0078.
Values may be sent and summed in bfloat16 or wider, within the bound.
A program may use at most 128 MiB of HBM per device.

```python
import math
import jax
import jax.numpy as jnp
import numpy as np
from jax import lax

D = 2048
FF = 2048
SPLIT = 4
FF_DEV = 512
TOP_K = 2
TOK_DEV = 128
EXPERTS = 16
CAP = 32
TOKENS = 8192
N_EP = 64


def levels(stream_key, extent, pieces, low, largest):
    factor_of, own = 1.0, jax.random.fold_in(stream_key, 6)
    for position, shards_of in pieces:
        steps = jnp.exp(jax.random.uniform(jax.random.fold_in(own, position), (shards_of,), jnp.float32, low / len(pieces), largest / len(pieces)))
        factor_of = factor_of * jnp.repeat(steps, extent[position] // shards_of).reshape([-1 if axis == position else 1 for axis in range(len(extent))])
    return factor_of


def assign_block(own_key, own, number, rows, amount, top, bound, skew):
    sequence = jax.random.permutation(own_key, amount)
    crowded, ordinary = shares(amount, rows * top, bound, skew, True), shares(amount, rows * top, bound, skew, False)
    places = jnp.arange(amount)

    def named(tallies, turn):
        used = int((tallies > 0).sum())
        fixed = max(1, used // 4)
        shifted = fixed + (places - fixed + turn * (used - fixed)) % max(1, amount - fixed)
        return jnp.zeros((amount,), jnp.int32).at[sequence[jnp.where(places < fixed, places, shifted)]].set(jnp.asarray(tallies, jnp.int32))

    tallies = jnp.where(number % 4 == 0, named(crowded, number // 4), named(ordinary, number - number // 4 - 1))
    mixed = jax.random.permutation(jax.random.fold_in(own, 3), amount)
    source_of, receiver = mixed[0:amount // 2 * 2:2], mixed[1:amount // 2 * 2:2]
    margin = jnp.minimum(tallies[source_of] - 1, bound - tallies[receiver]) // 2
    margin = jnp.where((source_of == sequence[0]) | (receiver == sequence[0]) | (tallies[receiver] == 0), 0, jnp.maximum(margin, 0))
    shifted = jax.random.randint(jax.random.fold_in(own, 4), (amount // 2,), 0, 1 << 20) % (margin + 1)
    tallies = tallies.at[source_of].add(-shifted).at[receiver].add(shifted)
    items = jnp.searchsorted(jnp.cumsum(tallies), jnp.arange(rows * top), side="right").astype(jnp.int32)
    table = items.reshape(top, rows).T
    table = table[jax.random.permutation(jax.random.fold_in(own, 1), rows)]
    turn = jax.random.randint(jax.random.fold_in(own, 2), (rows, 1), 0, top)
    return jnp.take_along_axis(table, (jnp.arange(top)[None, :] + turn) % top, axis=1)


def shares(amount, total, limit, slope, full):
    loads = [(1 << 20) // math.isqrt(rank ** slope) + 1 for rank in range(1, amount + 1)]
    largest = limit if full else min(limit, max(-(-total // amount), total * loads[0] // sum(loads)))
    least = 1 if total - largest >= amount - 1 else 0
    holding, rest = [largest] + [least] * (amount - 1), total - largest - least * (amount - 1)
    while rest > 0:
        candidates = [i for i in range(1, amount) if holding[i] < largest] or [i for i in range(1, amount) if holding[i] < limit]
        whole, budget = sum([loads[i] for i in candidates]), rest
        for i in candidates:
            extra = min(limit - holding[i], max(1, budget * loads[i] // whole), rest)
            holding[i] = holding[i] + extra
            rest = rest - extra
    return np.array(holding)


def normal_values(stream_key, dims, width, reach, cuts=(), held_as=jnp.bfloat16):
    drawn = width * jax.random.normal(stream_key, dims, jnp.float32)
    if cuts:
        drawn = drawn * levels(stream_key, dims, cuts, -0.22, 0.18)
    return jnp.clip(drawn, -reach, reach).astype(held_as)


def setup_inputs(seed: int = 0, part: int = 0) -> dict:
    key_list = jax.random.split(jax.random.key(seed), 8)
    part_keys = jax.random.split(jax.random.fold_in(key_list[7], part), 8)
    tokens = normal_values(part_keys[0], (TOKENS, D), 1.0, 6.0, ((0, 64),))
    norm_gain = jnp.clip(1.0 + 0.18 * jax.random.normal(key_list[1], (D,), jnp.float32), 0.1, 1.9)
    expert_ids_keys = jax.random.split(jax.random.fold_in(part_keys[2], 1), TOKENS // TOK_DEV)
    expert_ids_turns = jax.random.permutation(jax.random.fold_in(part_keys[2], 3), TOKENS // TOK_DEV)
    expert_ids = jax.vmap(lambda own, number: assign_block(jax.random.fold_in(part_keys[2], 2), own, number, TOK_DEV, EXPERTS, TOP_K, CAP, 2))(expert_ids_keys, expert_ids_turns).reshape((TOKENS, TOP_K))
    route_weight = jnp.clip(jnp.exp(math.log(1.0) - 2.3025851 * jax.random.uniform(part_keys[3], (TOKENS, TOP_K), jnp.float32) ** levels(part_keys[3], (TOKENS, TOP_K), ((0, 64),), -0.2, 0.2)), 0.1, 1.0)
    gate_weight = normal_values(key_list[4], (N_EP, D, FF_DEV), (D // 8) ** -0.5, 0.375, ((0, 64),))
    up_weight = normal_values(key_list[5], (N_EP, D, FF_DEV), (D // 8) ** -0.5, 0.375, ((0, 64),))
    down_weight = normal_values(key_list[6], (N_EP, FF_DEV, D), (16 * FF) ** -0.5, 0.03125, ((0, 64),))
    return dict(tokens=tokens, norm_gain=norm_gain, expert_ids=expert_ids, route_weight=route_weight, gate_weight=gate_weight, up_weight=up_weight, down_weight=down_weight)


EPSILON = 1e-05
clamp_limit = 7.0
sigmoid_slope = 1.702
row_block = 256

def reference(tokens, norm_gain, expert_ids, route_weight, gate_weight, up_weight, down_weight):
    values = tokens.astype(jnp.float32)
    center = values - lax.optimization_barrier(jnp.mean(values, axis=-1, keepdims=True))
    spread = lax.optimization_barrier(jnp.mean(center * center, axis=-1, keepdims=True))
    normed = (center * lax.rsqrt(spread + EPSILON) * norm_gain).astype(jnp.bfloat16)
    w_gate = gate_weight.reshape(EXPERTS, SPLIT, D, FF_DEV).transpose(0, 2, 1, 3).reshape(EXPERTS, D, FF)
    w_up = up_weight.reshape(EXPERTS, SPLIT, D, FF_DEV).transpose(0, 2, 1, 3).reshape(EXPERTS, D, FF)
    w_down = down_weight.reshape(EXPERTS, FF, D)
    assigned = TOKENS * TOP_K
    flat_ids = expert_ids.reshape(assigned).astype(jnp.int32)
    owners = jnp.arange(assigned, dtype=jnp.int32) // TOP_K
    ranking = jnp.argsort(flat_ids, stable=True).astype(jnp.int32)
    sorted_ids = flat_ids[ranking]
    counts = lax.optimization_barrier(jnp.sum((flat_ids[:, None] == jnp.arange(EXPERTS, dtype=jnp.int32)[None, :]).astype(jnp.int32), axis=0))
    starts = jnp.cumsum(counts) - counts
    padded_counts = (counts + row_block - 1) // row_block * row_block
    block_ends = jnp.cumsum(padded_counts)
    begins = block_ends - padded_counts
    target = (begins[sorted_ids] + jnp.arange(assigned, dtype=jnp.int32) - starts[sorted_ids]).astype(jnp.int32)
    blocks = -(-assigned // row_block) + EXPERTS
    slot_token = jnp.full((blocks * row_block,), TOKENS, jnp.int32).at[target].set(owners[ranking])
    first_rows = jnp.arange(blocks, dtype=jnp.int32) * row_block
    block_expert = jnp.minimum(lax.optimization_barrier(jnp.sum((first_rows[:, None] >= block_ends[None, :]).astype(jnp.int32), axis=1)), EXPERTS - 1).astype(jnp.int32)
    padded = jnp.concatenate([normed, jnp.zeros((1, D), jnp.bfloat16)], axis=0)
    gathered_rows = jnp.take(padded, slot_token, axis=0).reshape(blocks, row_block, D)

    def block_fn(operands):
        block_rows, expert = operands
        gate_pre = jnp.dot(block_rows, w_gate[expert], preferred_element_type=jnp.float32)
        up_pre = jnp.dot(block_rows, w_up[expert], preferred_element_type=jnp.float32)
        gate_cut = jnp.minimum(gate_pre, clamp_limit)
        up_cut = jnp.clip(up_pre, -clamp_limit, clamp_limit)
        active = ((up_cut + 1.0) * (gate_cut * jax.nn.sigmoid(gate_cut * sigmoid_slope))).astype(jnp.bfloat16)
        return jnp.dot(active, w_down[expert], preferred_element_type=jnp.float32).astype(jnp.bfloat16)
    outputs = lax.map(block_fn, (gathered_rows, block_expert)).reshape(blocks * row_block, D)
    sorted_out = jnp.take(outputs, target, axis=0)
    picked = jnp.zeros((assigned, D), jnp.bfloat16).at[ranking].set(sorted_out).reshape(TOKENS, TOP_K, D)
    combined = lax.optimization_barrier(jnp.sum(route_weight[:, :, None] * picked.astype(jnp.float32), axis=1))
    return combined.astype(jnp.bfloat16)
```

```python
import functools

import jax
import jax.numpy as jnp
from jax import lax
from jax.experimental import pallas as pl
from jax.experimental.pallas import tpu as pltpu
from jax.sharding import PartitionSpec as P

SPLIT = 4
CORES = 2

EPSILON = 1e-05
clamp_limit = 7.0
sigmoid_slope = 1.702
MESH = pl.DeviceIdType.MESH
F32 = jnp.float32
BF16 = jnp.bfloat16


def kernel(
    devices,
    tokens_ref,
    gain_ref,
    ids_col_ref,
    ids_row_ref,
    weight_col_ref,
    gate_hbm,
    up_hbm,
    down_hbm,
    out_ref,
    ring,
    back,
    meta,
    rows_in,
    own_part,
    sent_part,
    part_in,
    active,
    normed,
    unsort,
    added,
    gate,
    up,
    down,
    load_sem,
    ring_send,
    ring_recv,
    meta_send,
    meta_recv,
    rows_send,
    rows_recv,
    part_send,
    part_recv,
    back_send,
    back_recv,
):
    tok, width = tokens_ref.shape
    hidden = gate.shape[1]
    experts = devices // SPLIT
    side = experts // 2
    cap = min(tok, 2 * tok * ids_col_ref.shape[1] // experts)
    far = devices // CORES // 2
    half = tok // 2
    sizes = [cap * i for i in range(1, half // cap + 1)]
    pair = 2 * cap

    me = lax.axis_index("ep")
    chip = lax.div(me, CORES)
    core = lax.rem(me, CORES)
    sibling = me + 1 - 2 * core
    upper = lax.rem(me + CORES, devices)
    lower = lax.rem(me + devices - CORES, devices)
    parity = lax.rem(chip, 2)
    expert = lax.div(chip, SPLIT // CORES)
    first_code = (expert * cap).astype(F32)

    loads = [
        pltpu.make_async_copy(src.at[0], dst, load_sem.at[i])
        for i, (src, dst) in enumerate(((gate_hbm, gate), (up_hbm, up), (down_hbm, down)))
    ]
    for load in loads:
        load.start()

    def late(way, k):
        odd = lax.rem(chip + k, 2)
        return 1 - odd if way == 0 else odd

    def count(k, offset):
        left = cap * (side - lax.div(k + offset, 2))
        return jnp.minimum(tok, jnp.maximum(left, 0))

    def each_piece(rows, h, act):
        piece = jnp.clip(rows - half * h, 0, half)
        for size in sizes:

            @pl.when(piece == size)
            def _():
                act(size)

    def ring_copy(way, k, h, size):
        span = pl.ds(half * h, size)
        return pltpu.make_async_remote_copy(
            src_ref=ring.at[way, k, span],
            dst_ref=ring.at[way, k + 1, span],
            send_sem=ring_send.at[way, h, k],
            recv_sem=ring_recv.at[way, h, k + 1],
            device_id={"ep": upper if way == 0 else lower},
            device_id_type=MESH,
        )

    def meta_copy(way, k):
        return pltpu.make_async_remote_copy(
            src_ref=meta.at[way, k],
            dst_ref=meta.at[way, k + 1],
            send_sem=meta_send.at[way, k],
            recv_sem=meta_recv.at[way, k + 1],
            device_id={"ep": upper if way == 0 else lower},
            device_id_type=MESH,
        )

    def back_copy(way, k, h, size):
        span = pl.ds(half * h, size)
        return pltpu.make_async_remote_copy(
            src_ref=back.at[way, k, span],
            dst_ref=back.at[way, k - 1, span],
            send_sem=back_send.at[way, h, k],
            recv_sem=back_recv.at[way, h, k - 1],
            device_id={"ep": lower if way == 0 else upper},
            device_id_type=MESH,
        )

    def rows_copy(k):
        return pltpu.make_async_remote_copy(
            src_ref=rows_in.at[k, pl.ds(0, pair)],
            dst_ref=rows_in.at[k, pl.ds(pair, pair)],
            send_sem=rows_send.at[k],
            recv_sem=rows_recv.at[k],
            device_id={"ep": sibling},
            device_id_type=MESH,
        )

    def part_copy(k):
        return pltpu.make_async_remote_copy(
            src_ref=sent_part.at[lax.rem(k, 2)],
            dst_ref=part_in.at[k],
            send_sem=part_send.at[k],
            recv_sem=part_recv.at[k],
            device_id={"ep": sibling},
            device_id_type=MESH,
        )

    shrink = 2 * (side - tok // cap)

    @pl.loop(shrink, far + 1)
    def _(k):
        for way in range(2):
            ring[way, k] = jnp.zeros((tok, width), BF16)
            meta[way, k] = jnp.full(meta.shape[2:], -1.0, F32)

    barrier = pltpu.get_barrier_semaphore()
    for peer in (upper, lower, sibling):
        pl.semaphore_signal(barrier, inc=1, device_id={"ep": peer}, device_id_type=MESH)

    block = min(tok, 32)

    @pl.loop(0, tok // block)
    def _(i):
        span = pl.ds(pl.multiple_of(i * block, block), block)
        values = tokens_ref[span, :].astype(F32)
        center = values - jnp.mean(values, axis=-1, keepdims=True)
        spread = jnp.mean(center * center, axis=-1, keepdims=True)
        normed[span, :] = (center * lax.rsqrt(spread + EPSILON) * gain_ref[...]).astype(BF16)

    def reach(ids, way):
        offset = late(way, 0)
        steps = ids - expert if way == 0 else expert - ids
        steps = jnp.where(steps < 0, steps + experts, steps)
        inside = (steps >= 1 - offset) & (steps <= side - offset)
        return jnp.where(inside, 2 * steps + offset, 0)

    row_index = lax.broadcasted_iota(jnp.int32, (tok, tok), 0)
    col_index = lax.broadcasted_iota(jnp.int32, (tok, tok), 1)
    id_col = [ids_col_ref[:, i : i + 1] for i in range(2)]
    id_row = [ids_row_ref[i : i + 1, :] for i in range(2)]
    weight_col = [weight_col_ref[:, i : i + 1] for i in range(2)]
    code_col = []
    for i in range(2):
        same = ((id_row[0] == id_col[i]) | (id_row[1] == id_col[i])) & (col_index < row_index)
        slot = jnp.sum(jnp.where(same, 1.0, 0.0), axis=1, keepdims=True)
        code_col.append(id_col[i].astype(F32) * float(cap) + slot)
    facts = (code_col[0], code_col[1], weight_col[0], weight_col[1])
    sorts = []
    for way in range(2):
        key_col = jnp.maximum(reach(id_col[0], way), reach(id_col[1], way))
        key_row = jnp.maximum(reach(id_row[0], way), reach(id_row[1], way))
        ahead = (key_row > key_col) | ((key_row == key_col) & (col_index < row_index))
        rank_col = jnp.sum(jnp.where(ahead, 1.0, 0.0), axis=1, keepdims=True).astype(jnp.int32)
        behind = (key_col > key_row) | ((key_col == key_row) & (row_index < col_index))
        rank_row = jnp.sum(jnp.where(behind, 1.0, 0.0), axis=0, keepdims=True).astype(jnp.int32)
        placed = col_index == rank_col
        unsort[way] = jnp.where(placed, 1.0, 0.0).astype(BF16)
        for i, fact in enumerate(facts):
            meta[way, 0, i : i + 1, :] = jnp.sum(
                jnp.where(placed, fact, 0.0), axis=0, keepdims=True
            )
        sorts.append(jnp.where(row_index == rank_row, 1.0, 0.0).astype(BF16))
    for way in range(2):
        ring[way, 0] = jnp.dot(
            sorts[way], normed[...], preferred_element_type=F32
        ).astype(BF16)

    pl.semaphore_wait(barrier, 3)

    def matches(way, k):
        slots = lax.broadcasted_iota(jnp.int32, (cap, tok), 0).astype(F32) + first_code
        return meta[way, k, 0:1, :] == slots, meta[way, k, 1:2, :] == slots

    def onehot(way, k):
        first, second = matches(way, k)
        return jnp.where(first | second, 1.0, 0.0).astype(BF16)

    def pass_on(k, h):
        for way in range(2):
            offset = late(way, k)
            rows = jnp.where(k > 0, count(k - 1, offset), 0)
            each_piece(rows, h, lambda size: ring_copy(way, k - 1, h, size).wait_recv())
            each_piece(count(k, offset), h, lambda size: ring_copy(way, k, h, size).start())
            if h == 0:

                @pl.when(rows > 0)
                def _():
                    meta_copy(way, k - 1).wait_recv()

                @pl.when(count(k, offset) > 0)
                def _():
                    meta_copy(way, k).start()

    def select(k):
        for way in range(2):
            rows_in[k, way * cap : (way + 1) * cap] = jnp.dot(
                onehot(way, k), ring[way, k], preferred_element_type=F32
            ).astype(BF16)
        rows_copy(k).start()

    def hidden_units(k):
        rows_copy(k).wait_recv()
        block_rows = rows_in[k]
        gate_pre = jnp.dot(block_rows, gate[...], preferred_element_type=F32)
        up_pre = jnp.dot(block_rows, up[...], preferred_element_type=F32)
        gate_cut = jnp.minimum(gate_pre, clamp_limit)
        up_cut = jnp.clip(up_pre, -clamp_limit, clamp_limit)
        active[...] = (
            (up_cut + 1.0) * (gate_cut * jax.nn.sigmoid(gate_cut * sigmoid_slope))
        ).astype(BF16)

    def outputs(k):
        slot = lax.rem(k, 2)

        @pl.when(k >= 2)
        def _():
            part_copy(k - 2).wait_send()

        for start in range(0, width, hidden):
            span = slice(start, start + hidden)
            partial = jnp.dot(active[...], down[:, span], preferred_element_type=F32)
            own_part[slot, :, span] = partial[:pair]
            sent_part[slot, :, span] = partial[pair:].astype(BF16)
        part_copy(k).start()

    def weigh(k):
        part_copy(k).wait_recv()
        slot = lax.rem(k, 2)
        for way in range(2):
            first, second = matches(way, k)
            scale = jnp.sum(
                jnp.where(first, meta[way, k, 2:3, :], 0.0)
                + jnp.where(second, meta[way, k, 3:4, :], 0.0),
                axis=1,
                keepdims=True,
            )
            span = slice(way * cap, (way + 1) * cap)
            whole = own_part[slot, span] + part_in[k, span].astype(F32)
            part_in[k, span] = (whole * scale).astype(BF16)

    @pl.loop(0, far + 3)
    def _(k):
        pl.when(k <= far)(lambda: pass_on(k, 0))

        @pl.when((k >= 1) & (k <= far + 1))
        def _():
            @pl.when(k == 1)
            def _():
                for load in loads:
                    load.wait()

            hidden_units(k - 1)

        @pl.when(k <= far)
        def _():
            pass_on(k, 1)
            select(k)

        pl.when((k >= 1) & (k <= far + 1))(lambda: outputs(k - 1))
        pl.when(k >= 2)(lambda: weigh(k - 2))

    def spread_rows(way, k):
        return lax.dot_general(
            onehot(way, k),
            part_in[k, way * cap : (way + 1) * cap],
            (((0,), (0,)), ((), ())),
            preferred_element_type=F32,
        )

    @pl.loop(0, far)
    def _(i):
        k = far - i
        for way in range(2):
            added[way] = spread_rows(way, k).astype(BF16)
        for h in range(2):
            for way in range(2):
                offset = late(way, k)
                held = count(k, offset)
                each_piece(held, h, lambda size: back_copy(way, k + 1, h, size).wait_recv())

                def send(size):
                    span = pl.ds(half * h, size)
                    index = lax.broadcasted_iota(jnp.int32, (size, 1), 0) + half * h
                    before = jnp.where(index < held, back[way, k, span].astype(F32), 0.0)
                    back[way, k, span] = (before + added[way, span].astype(F32)).astype(BF16)
                    back_copy(way, k, h, size).start()

                each_piece(count(k - 1, offset), h, send)

    for h in range(2):
        for way in range(2):
            back_copy(way, 1, h, half).wait_recv()
    total = spread_own = None
    total = lax.dot_general(
        onehot(0, 0),
        part_in[0, 0:cap],
        (((0,), (0,)), ((), ())),
        preferred_element_type=F32,
    )
    own = lax.dot_general(
        unsort[0], total.astype(BF16), (((1,), (0,)), ((), ())), preferred_element_type=F32
    )
    for way in range(2):
        own = own + jnp.dot(unsort[way], back[way, 0], preferred_element_type=F32)
    out_ref[...] = own.astype(BF16)

    @pl.loop(0, far + 1)
    def _(k):
        rows_copy(k).wait_send()
        pl.when(k >= far - 1)(lambda: part_copy(k).wait_send())
        for way in range(2):
            offset = late(way, k)
            rows = count(k, offset)

            @pl.when(rows > 0)
            def _():
                meta_copy(way, k).wait_send()

            for h in range(2):
                each_piece(rows, h, lambda size: ring_copy(way, k, h, size).wait_send())
                sent = jnp.where(k > 0, count(k - 1, offset), 0)
                each_piece(sent, h, lambda size: back_copy(way, k, h, size).wait_send())


def body(tokens, norm_gain, expert_ids, route_weight, gate_weight, up_weight, down_weight):
    devices = lax.axis_size("ep")
    tok, width = tokens.shape
    top_count = expert_ids.shape[1]
    hidden = gate_weight.shape[2]
    experts = devices // SPLIT
    cap = min(tok, 2 * tok * top_count // experts)
    far = devices // CORES // 2
    steps = far + 1
    vmem = pl.BlockSpec(memory_space=pltpu.VMEM)
    hbm = pl.BlockSpec(memory_space=pl.ANY)
    dma = pltpu.SemaphoreType.DMA
    return pl.pallas_call(
        functools.partial(kernel, devices),
        out_shape=jax.ShapeDtypeStruct((tok, width), BF16),
        in_specs=[vmem] * 5 + [hbm] * 3,
        out_specs=vmem,
        scratch_shapes=[
            pltpu.VMEM((2, steps, tok, width), BF16),
            pltpu.VMEM((2, steps, tok, width), BF16),
            pltpu.VMEM((2, steps, 8, tok), F32),
            pltpu.VMEM((steps, 4 * cap, width), BF16),
            pltpu.VMEM((2, 2 * cap, width), F32),
            pltpu.VMEM((2, 2 * cap, width), BF16),
            pltpu.VMEM((steps, 2 * cap, width), BF16),
            pltpu.VMEM((4 * cap, hidden), BF16),
            pltpu.VMEM((tok, width), BF16),
            pltpu.VMEM((2, tok, tok), BF16),
            pltpu.VMEM((2, tok, width), BF16),
            pltpu.VMEM((width, hidden), BF16),
            pltpu.VMEM((width, hidden), BF16),
            pltpu.VMEM((hidden, width), BF16),
            dma((3,)),
            dma((2, 2, steps)),
            dma((2, 2, steps)),
            dma((2, steps)),
            dma((2, steps)),
            dma((steps,)),
            dma((steps,)),
            dma((steps,)),
            dma((steps,)),
            dma((2, 2, steps)),
            dma((2, 2, steps)),
        ],
        compiler_params=pltpu.CompilerParams(
            collective_id=0, has_side_effects=True, vmem_limit_bytes=67043328
        ),
    )(
        tokens,
        norm_gain.reshape(1, width),
        expert_ids,
        expert_ids.T,
        route_weight,
        gate_weight,
        up_weight,
        down_weight,
    )


def solution(mesh):
    placed = (
        P(("grp", "ep"), None),
        P(),
        P(("grp", "ep"), None),
        P(("grp", "ep"), None),
        P("ep", None, None),
        P("ep", None, None),
        P("ep", None, None),
    )
    return jax.shard_map(
        body, mesh=mesh, in_specs=placed, out_specs=P(("grp", "ep"), None), check_vma=False
    )
```

```python
import functools

import jax
import jax.numpy as jnp
from jax import lax
from jax.experimental import pallas as pl
from jax.experimental.pallas import tpu as pltpu
from jax.sharding import PartitionSpec as P

SPLIT = 4
CORES = 2
WAVES = 2
LEAD = 11
SLOTS = 4

EPSILON = 1e-05
clamp_limit = 7.0
sigmoid_slope = 1.702
MESH = pl.DeviceIdType.MESH
F32 = jnp.float32
BF16 = jnp.bfloat16


def left_rows(tok, cap, side, k, offset):
    return min(tok, max(0, cap * (side - (k + offset) // 2)))


def plan(devices, tok, top_count):
    experts = devices // SPLIT
    side = experts // 2
    cap = min(tok, 2 * tok * top_count // experts)
    half = tok // WAVES
    radii, thin = [], []
    for w in range(WAVES):
        hops = range(1, devices // CORES + 1)
        radii.append(max(k for k in hops if left_rows(tok, cap, side, k - 1, 0) > w * half))
        full = (w + 1) * half
        thin.append(min(k for k in hops if left_rows(tok, cap, side, k - 1, 1) < full))
    return experts, side, cap, half, radii, thin


def kernel(
    devices,
    piece,
    tokens_ref,
    gain_ref,
    ids_ref,
    weight_ref,
    gate_hbm,
    up_hbm,
    down_hbm,
    out_ref,
    *scratch,
):
    waves = [scratch[i * 15 : (i + 1) * 15] for i in range(WAVES)]
    active, normed, gate, up, down, load_sem = scratch[WAVES * 15 :]
    (
        ring,
        back,
        meta,
        rows_in,
        own_part,
        sent_part,
        part_in,
        unsort,
        added,
        row_sem,
        part_sem,
        ring_send,
        ring_recv,
        back_send,
        back_recv,
    ) = zip(*waves)
    tok, width = tokens_ref.shape
    hidden = gate.shape[1]
    experts, side, cap, half, radii, thin = plan(devices, tok, ids_ref.shape[0])
    pair = 2 * cap
    pieces = half // piece
    starts = [w * LEAD for w in range(WAVES)]

    me = lax.axis_index("ep")
    chip = lax.div(me, CORES)
    core = lax.rem(me, CORES)
    sibling = me + 1 - 2 * core
    upper = lax.rem(me + CORES, devices)
    lower = lax.rem(me + devices - CORES, devices)
    expert = lax.div(chip, SPLIT // CORES)
    first_code = (expert * cap).astype(F32)

    loads = [
        pltpu.make_async_copy(src.at[0], dst, load_sem.at[i])
        for i, (src, dst) in enumerate(((gate_hbm, gate), (up_hbm, up), (down_hbm, down)))
    ]
    for load in loads:
        load.start()

    def late(way, k):
        odd = lax.rem(chip + k, 2)
        return 1 - odd if way == 0 else odd

    def count(k, offset):
        left = cap * (side - lax.div(k + offset, 2))
        return jnp.minimum(tok, jnp.maximum(left, 0))

    def goes(w, p, rows):
        return rows > w * half + p * piece

    def remote(src, dst, send, recv, peer):
        return pltpu.make_async_remote_copy(
            src_ref=src,
            dst_ref=dst,
            send_sem=send,
            recv_sem=recv,
            device_id={"ep": peer},
            device_id_type=MESH,
        )

    def ring_copy(w, way, k, p):
        span = pl.ds(p * piece, piece)
        return remote(
            ring[w].at[way, k, span],
            ring[w].at[way, k + 1, span],
            ring_send[w].at[way, p, k],
            ring_recv[w].at[way, p, k + 1],
            upper if way == 0 else lower,
        )

    def meta_copy(w, way, k):
        return remote(
            meta[w].at[way, k],
            meta[w].at[way, k + 1],
            ring_send[w].at[way, pieces, k],
            ring_recv[w].at[way, pieces, k + 1],
            upper if way == 0 else lower,
        )

    def back_copy(w, way, k, p):
        span = pl.ds(p * piece, piece)
        return remote(
            back[w].at[way, k, span],
            back[w].at[way, k - 1, span],
            back_send[w].at[way, p, k],
            back_recv[w].at[way, p, k - 1],
            lower if way == 0 else upper,
        )

    def rows_copy(w, k):
        slot = lax.rem(k, SLOTS)
        return remote(
            rows_in[w].at[slot, pl.ds(0, pair)],
            rows_in[w].at[slot, pl.ds(pair, pair)],
            row_sem[w].at[0, k],
            row_sem[w].at[1, k],
            sibling,
        )

    def part_copy(w, k):
        return remote(
            sent_part[w].at[lax.rem(k, 2)],
            part_in[w].at[k],
            part_sem[w].at[0, k],
            part_sem[w].at[1, k],
            sibling,
        )

    for w in range(WAVES):

        @pl.loop(thin[w], radii[w] + 1)
        def _(k):
            for way in range(2):
                ring[w][way, k] = jnp.zeros((half, width), BF16)
                meta[w][way, k] = jnp.full(meta[w].shape[2:], -1.0, F32)

    barrier = pltpu.get_barrier_semaphore()
    for peer in (upper, lower, sibling):
        pl.semaphore_signal(barrier, inc=1, device_id={"ep": peer}, device_id_type=MESH)

    block = min(tok, 32)

    @pl.loop(0, tok // block)
    def _(i):
        span = pl.ds(pl.multiple_of(i * block, block), block)
        values = tokens_ref[span, :].astype(F32)
        center = values - jnp.mean(values, axis=-1, keepdims=True)
        spread = jnp.mean(center * center, axis=-1, keepdims=True)
        normed[span, :] = (center * lax.rsqrt(spread + EPSILON) * gain_ref[...]).astype(BF16)

    def reach(ids, way):
        offset = late(way, 0)
        steps = ids - expert if way == 0 else expert - ids
        steps = jnp.where(steps < 0, steps + experts, steps)
        inside = (steps >= 1 - offset) & (steps <= side - offset)
        return jnp.where(inside, 2 * steps + offset, 0).astype(F32)

    row_index = lax.broadcasted_iota(jnp.int32, (tok, tok), 0)
    col_index = lax.broadcasted_iota(jnp.int32, (tok, tok), 1)
    diagonal = row_index == col_index

    def as_column(row):
        return jnp.sum(jnp.where(diagonal, row, 0.0), axis=1, keepdims=True)

    id_row = [ids_ref[i : i + 1, :] for i in range(2)]
    code_row = [ids.astype(F32) for ids in id_row]
    code_col = [as_column(code) for code in code_row]
    facts = []
    for i in range(2):
        same = (code_row[0] == code_col[i]) | (code_row[1] == code_col[i])
        slot = jnp.sum(
            jnp.where(same & (col_index < row_index), 1.0, 0.0), axis=1, keepdims=True
        )
        facts.append(code_col[i] * float(cap) + slot)
    facts += [as_column(weight_ref[i : i + 1, :]) for i in range(2)]
    for way in range(2):
        key_row = jnp.maximum(reach(id_row[0], way), reach(id_row[1], way))
        key_col = as_column(key_row)
        ahead = (key_row > key_col) | ((key_row == key_col) & (col_index < row_index))
        rank_col = jnp.sum(jnp.where(ahead, 1.0, 0.0), axis=1, keepdims=True).astype(jnp.int32)
        behind = (key_col > key_row) | ((key_col == key_row) & (row_index < col_index))
        rank_row = jnp.sum(jnp.where(behind, 1.0, 0.0), axis=0, keepdims=True).astype(jnp.int32)
        sort = jnp.where(row_index == rank_row, 1.0, 0.0).astype(BF16)
        ordered = jnp.dot(sort, normed[...], preferred_element_type=F32).astype(BF16)
        for w in range(WAVES):
            placed = col_index + w * half == rank_col
            unsort[w][way] = jnp.where(placed, 1.0, 0.0).astype(BF16)
            for i, fact in enumerate(facts):
                meta[w][way, 0, i : i + 1, :] = jnp.sum(
                    jnp.where(placed, fact, 0.0), axis=0, keepdims=True
                )
            ring[w][way, 0] = ordered[w * half : (w + 1) * half]

    pl.semaphore_wait(barrier, 3)

    def matches(w, way, k):
        slots = lax.broadcasted_iota(jnp.int32, (cap, half), 0).astype(F32) + first_code
        return meta[w][way, k, 0:1, 0:half] == slots, meta[w][way, k, 1:2, 0:half] == slots

    def onehot(w, way, k):
        first, second = matches(w, way, k)
        return jnp.where(first | second, 1.0, 0.0).astype(BF16)

    def pass_on(w, k):
        for way in range(2):
            offset = late(way, k)
            came = (k > 0) & goes(w, 0, count(k - 1, offset))
            pl.when(came)(lambda: meta_copy(w, way, k - 1).wait_recv())
            pl.when(goes(w, 0, count(k, offset)))(lambda: meta_copy(w, way, k).start())
        for p in range(pieces):
            for way in range(2):
                offset = late(way, k)
                came = (k > 0) & goes(w, p, count(k - 1, offset))
                pl.when(came)(lambda: ring_copy(w, way, k - 1, p).wait_recv())
                pl.when(goes(w, p, count(k, offset)))(lambda: ring_copy(w, way, k, p).start())

    def select(w, k):
        slot = lax.rem(k, SLOTS)
        pl.when(k >= SLOTS)(lambda: rows_copy(w, k - SLOTS).wait_send())
        for way in range(2):
            rows_in[w][slot, way * cap : (way + 1) * cap] = jnp.dot(
                onehot(w, way, k), ring[w][way, k], preferred_element_type=F32
            ).astype(BF16)
        rows_copy(w, k).start()

    def expert_rows(w, k):
        rows_copy(w, k).wait_recv()
        block_rows = rows_in[w][lax.rem(k, SLOTS)]
        gate_pre = jnp.dot(block_rows, gate[...], preferred_element_type=F32)
        up_pre = jnp.dot(block_rows, up[...], preferred_element_type=F32)
        gate_cut = jnp.minimum(gate_pre, clamp_limit)
        up_cut = jnp.clip(up_pre, -clamp_limit, clamp_limit)
        active[...] = (
            (up_cut + 1.0) * (gate_cut * jax.nn.sigmoid(gate_cut * sigmoid_slope))
        ).astype(BF16)
        slot = lax.rem(k, 2)
        pl.when(k >= 2)(lambda: part_copy(w, k - 2).wait_send())
        for start in range(0, width, hidden):
            span = slice(start, start + hidden)
            partial = jnp.dot(active[...], down[:, span], preferred_element_type=F32)
            own_part[w][slot, :, span] = partial[:pair]
            sent_part[w][slot, :, span] = partial[pair:].astype(BF16)
        part_copy(w, k).start()

    def weigh(w, k):
        part_copy(w, k).wait_recv()
        slot = lax.rem(k, 2)
        for way in range(2):
            first, second = matches(w, way, k)
            scale = jnp.sum(
                jnp.where(first, meta[w][way, k, 2:3, 0:half], 0.0)
                + jnp.where(second, meta[w][way, k, 3:4, 0:half], 0.0),
                axis=1,
                keepdims=True,
            )
            span = slice(way * cap, (way + 1) * cap)
            whole = own_part[w][slot, span] + part_in[w][k, span].astype(F32)
            part_in[w][k, span] = (whole * scale).astype(BF16)

    def spread_rows(w, way, k):
        return lax.dot_general(
            onehot(w, way, k),
            part_in[w][k, way * cap : (way + 1) * cap],
            (((0,), (0,)), ((), ())),
            preferred_element_type=F32,
        ).astype(BF16)

    def bring_back(w, k):
        for way in range(2):
            added[w][way] = spread_rows(w, way, k)
        for p in range(pieces):
            for way in range(2):
                offset = late(way, k)
                held = goes(w, p, count(k, offset))
                pl.when(held)(lambda: back_copy(w, way, k + 1, p).wait_recv())

                @pl.when(goes(w, p, count(k - 1, offset)))
                def _():
                    span = pl.ds(p * piece, piece)
                    before = jnp.where(held, back[w][way, k, span].astype(F32), 0.0)
                    back[w][way, k, span] = (before + added[w][way, span].astype(F32)).astype(BF16)
                    back_copy(w, way, k, p).start()

    def within(value, low, high):
        return (value >= low) & (value <= high)

    @pl.loop(0, max(s + 2 * r for s, r in zip(starts, radii)) + 3)
    def _(i):
        for w in range(WAVES):
            k = i - starts[w]
            pl.when(within(k, 0, radii[w]))(lambda: pass_on(w, k))
            home = 2 * radii[w] + 3 - k
            pl.when(within(home, 1, radii[w]))(lambda: bring_back(w, home))

        @pl.when(i == 1)
        def _():
            for load in loads:
                load.wait()

        for w in range(WAVES):
            k = i - starts[w]
            pl.when(within(k, 1, radii[w] + 1))(lambda: expert_rows(w, k - 1))
            pl.when(within(k, 0, radii[w]))(lambda: select(w, k))
            pl.when(within(k, 2, radii[w] + 2))(lambda: weigh(w, k - 2))

    total = None
    for w in range(WAVES):
        for p in range(pieces):
            for way in range(2):
                back_copy(w, way, 1, p).wait_recv()
        for way, rows in ((0, spread_rows(w, 0, 0)), (0, back[w][0, 0]), (1, back[w][1, 0])):
            share = jnp.dot(unsort[w][way, :, 0:half], rows, preferred_element_type=F32)
            total = share if total is None else total + share
    out_ref[...] = total.astype(BF16)

    for w in range(WAVES):

        @pl.loop(0, radii[w] + 1)
        def _(k):
            pl.when(k > radii[w] - SLOTS)(lambda: rows_copy(w, k).wait_send())
            pl.when(k > radii[w] - 2)(lambda: part_copy(w, k).wait_send())
            for way in range(2):
                offset = late(way, k)
                rows = count(k, offset)
                pl.when(goes(w, 0, rows))(lambda: meta_copy(w, way, k).wait_send())
                for p in range(pieces):
                    pl.when(goes(w, p, rows))(lambda: ring_copy(w, way, k, p).wait_send())
                    sent = (k > 0) & goes(w, p, count(k - 1, offset))
                    pl.when(sent)(lambda: back_copy(w, way, k, p).wait_send())


def body(tokens, norm_gain, expert_ids, route_weight, gate_weight, up_weight, down_weight):
    devices = lax.axis_size("ep")
    tok, width = tokens.shape
    hidden = gate_weight.shape[2]
    experts, side, cap, half, radii, thin = plan(devices, tok, expert_ids.shape[1])
    piece = cap
    vmem = pl.BlockSpec(memory_space=pltpu.VMEM)
    hbm = pl.BlockSpec(memory_space=pl.ANY)
    dma = pltpu.SemaphoreType.DMA
    scratch = []
    for radius in radii:
        steps = radius + 1
        scratch += [
            pltpu.VMEM((2, steps, half, width), BF16),
            pltpu.VMEM((2, steps, half, width), BF16),
            pltpu.VMEM((2, steps, 8, tok), F32),
            pltpu.VMEM((SLOTS, 4 * cap, width), BF16),
            pltpu.VMEM((2, 2 * cap, width), F32),
            pltpu.VMEM((2, 2 * cap, width), BF16),
            pltpu.VMEM((steps, 2 * cap, width), BF16),
            pltpu.VMEM((2, tok, tok), BF16),
            pltpu.VMEM((2, half, width), BF16),
            dma((2, steps)),
            dma((2, steps)),
            dma((2, half // piece + 1, steps)),
            dma((2, half // piece + 1, steps)),
            dma((2, half // piece, steps)),
            dma((2, half // piece, steps)),
        ]
    scratch += [
        pltpu.VMEM((4 * cap, hidden), BF16),
        pltpu.VMEM((tok, width), BF16),
        pltpu.VMEM((width, hidden), BF16),
        pltpu.VMEM((width, hidden), BF16),
        pltpu.VMEM((hidden, width), BF16),
        dma((3,)),
    ]
    return pl.pallas_call(
        functools.partial(kernel, devices, piece),
        out_shape=jax.ShapeDtypeStruct((tok, width), BF16),
        in_specs=[vmem] * 4 + [hbm] * 3,
        out_specs=vmem,
        scratch_shapes=scratch,
        compiler_params=pltpu.CompilerParams(
            collective_id=0, has_side_effects=True, vmem_limit_bytes=67043328
        ),
    )(
        tokens,
        norm_gain.reshape(1, width),
        expert_ids.T,
        route_weight.T,
        gate_weight,
        up_weight,
        down_weight,
    )


def solution(mesh):
    placed = (
        P(("grp", "ep"), None),
        P(),
        P(("grp", "ep"), None),
        P(("grp", "ep"), None),
        P("ep", None, None),
        P("ep", None, None),
        P("ep", None, None),
    )
    return jax.shard_map(
        body, mesh=mesh, in_specs=placed, out_specs=P(("grp", "ep"), None), check_vma=False
    )
```

```python
import functools

import jax
import jax.numpy as jnp
from jax import lax
from jax.experimental import pallas as pl
from jax.experimental.pallas import tpu as pltpu
from jax.sharding import PartitionSpec as P

SPLIT = 4
CORES = 2
WAVES = 2
LEAD = 11
SLOTS = 4

EPSILON = 1e-05
clamp_limit = 7.0
sigmoid_slope = 1.702
MESH = pl.DeviceIdType.MESH
F32 = jnp.float32
BF16 = jnp.bfloat16


def left_rows(tok, cap, side, k, offset):
    return min(tok, max(0, cap * (side - (k + offset) // 2)))


def plan(devices, tok, top_count):
    experts = devices // SPLIT
    side = experts // 2
    cap = min(tok, 2 * tok * top_count // experts)
    half = tok // WAVES
    radii, thin = [], []
    for w in range(WAVES):
        hops = range(1, devices // CORES + 1)
        radii.append(max(k for k in hops if left_rows(tok, cap, side, k - 1, 0) > w * half))
        full = (w + 1) * half
        thin.append(min(k for k in hops if left_rows(tok, cap, side, k - 1, 1) < full))
    return experts, side, cap, half, radii, thin


def kernel(
    devices,
    piece,
    tokens_hbm,
    gain_ref,
    ids_ref,
    weight_ref,
    gate_hbm,
    up_hbm,
    down_hbm,
    out_ref,
    *scratch,
):
    waves = [scratch[i * 14 : (i + 1) * 14] for i in range(WAVES)]
    active, tokens, normed, sort, rows, gate, up, down, load_sem = scratch[WAVES * 14 :]
    (
        ring,
        back,
        meta,
        rows_in,
        own_part,
        sent_part,
        part_in,
        added,
        row_sem,
        part_sem,
        ring_send,
        ring_recv,
        back_send,
        back_recv,
    ) = zip(*waves)
    tok, width = tokens.shape
    hidden = gate.shape[1]
    experts, side, cap, half, radii, thin = plan(devices, tok, ids_ref.shape[0])
    pair = 2 * cap
    pieces = half // piece
    starts = [w * LEAD for w in range(WAVES)]

    me = lax.axis_index("ep")
    chip = lax.div(me, CORES)
    core = lax.rem(me, CORES)
    sibling = me + 1 - 2 * core
    upper = lax.rem(me + CORES, devices)
    lower = lax.rem(me + devices - CORES, devices)
    expert = lax.div(chip, SPLIT // CORES)
    first_code = (expert * cap).astype(F32)

    fetch = pltpu.make_async_copy(tokens_hbm, tokens, load_sem.at[3])
    fetch.start()
    loads = [
        pltpu.make_async_copy(src.at[0], dst, load_sem.at[i])
        for i, (src, dst) in enumerate(((gate_hbm, gate), (up_hbm, up), (down_hbm, down)))
    ]
    for load in loads:
        load.start()

    def late(way, k):
        odd = lax.rem(chip + k, 2)
        return 1 - odd if way == 0 else odd

    def count(k, offset):
        left = cap * (side - lax.div(k + offset, 2))
        return jnp.minimum(tok, jnp.maximum(left, 0))

    def goes(w, p, rows):
        return rows > w * half + p * piece

    def remote(src, dst, send, recv, peer):
        return pltpu.make_async_remote_copy(
            src_ref=src,
            dst_ref=dst,
            send_sem=send,
            recv_sem=recv,
            device_id={"ep": peer},
            device_id_type=MESH,
        )

    def ring_copy(w, way, k, p):
        span = pl.ds(p * piece, piece)
        return remote(
            ring[w].at[way, k, span],
            ring[w].at[way, k + 1, span],
            ring_send[w].at[way, p, k],
            ring_recv[w].at[way, p, k + 1],
            upper if way == 0 else lower,
        )

    def meta_copy(w, way, k):
        return remote(
            meta[w].at[way, k],
            meta[w].at[way, k + 1],
            ring_send[w].at[way, pieces, k],
            ring_recv[w].at[way, pieces, k + 1],
            upper if way == 0 else lower,
        )

    def back_copy(w, way, k, p):
        span = pl.ds(p * piece, piece)
        return remote(
            back[w].at[way, k, span],
            back[w].at[way, k - 1, span],
            back_send[w].at[way, p, k],
            back_recv[w].at[way, p, k - 1],
            lower if way == 0 else upper,
        )

    def rows_copy(w, k):
        slot = lax.rem(k, SLOTS)
        return remote(
            rows_in[w].at[slot, pl.ds(0, pair)],
            rows_in[w].at[slot, pl.ds(pair, pair)],
            row_sem[w].at[0, k],
            row_sem[w].at[1, k],
            sibling,
        )

    def part_copy(w, k):
        return remote(
            sent_part[w].at[lax.rem(k, 2)],
            part_in[w].at[k],
            part_sem[w].at[0, k],
            part_sem[w].at[1, k],
            sibling,
        )

    for w in range(WAVES):

        @pl.loop(thin[w], radii[w] + 1)
        def _(k):
            for way in range(2):
                ring[w][way, k] = jnp.zeros((half, width), BF16)
                meta[w][way, k] = jnp.full(meta[w].shape[2:], -1.0, F32)

    barrier = pltpu.get_barrier_semaphore()
    for peer in (upper, lower, sibling):
        pl.semaphore_signal(barrier, inc=1, device_id={"ep": peer}, device_id_type=MESH)

    def reach(ids, way):
        offset = late(way, 0)
        steps = ids - expert if way == 0 else expert - ids
        steps = jnp.where(steps < 0, steps + experts, steps)
        inside = (steps >= 1 - offset) & (steps <= side - offset)
        return jnp.where(inside, 2 * steps + offset, 0).astype(F32)

    def across(left, right):
        return lax.dot_general(left, right, (((1,), (1,)), ((), ())), preferred_element_type=F32)

    row_index = lax.broadcasted_iota(jnp.int32, (tok, tok), 0)
    col_index = lax.broadcasted_iota(jnp.int32, (tok, tok), 1)
    earlier = row_index < col_index
    ids = [ids_ref[i : i + 1, :] for i in range(2)]
    id_row = [each.astype(F32) for each in ids]
    key_row = [jnp.maximum(reach(ids[0], way), reach(ids[1], way)) for way in range(2)]
    rows[...] = jnp.zeros_like(rows)
    for i, row in enumerate((*id_row, *key_row)):
        rows[i : i + 1, :] = row
    identity = jnp.where(row_index == col_index, 1.0, 0.0).astype(BF16)
    columns = across(identity, rows[...].astype(BF16))
    id_col = [columns[:, i : i + 1] for i in range(2)]
    for way in range(2):
        key_col = columns[:, 2 + way : 3 + way]
        behind = (key_col > key_row[way]) | ((key_col == key_row[way]) & earlier)
        rank = jnp.sum(jnp.where(behind, 1.0, 0.0), axis=0, keepdims=True).astype(jnp.int32)
        sort[way] = jnp.where(row_index == rank, 1.0, 0.0).astype(BF16)
    for i in range(2):
        same = ((id_col[0] == id_row[i]) | (id_col[1] == id_row[i])) & earlier
        rows[i : i + 1, :] = id_row[i]
        rows[2 + i : 3 + i, :] = jnp.sum(jnp.where(same, 1.0, 0.0), axis=0, keepdims=True)
        rest = weight_ref[i : i + 1, :]
        for j in range(3):
            high = rest.astype(BF16).astype(F32)
            rows[4 + 3 * i + j : 5 + 3 * i + j, :] = high
            rest = rest - high
    facts = rows[...].astype(BF16)
    for w in range(WAVES):
        for way in range(2):
            sorted_facts = across(facts, sort[way, w * half : (w + 1) * half, :])
            fact = [sorted_facts[i : i + 1] for i in range(10)]
            meta[w][way, 0] = jnp.full(meta[w].shape[2:], -1.0, F32)
            for i in range(2):
                meta[w][way, 0, i : i + 1, 0:half] = fact[i] * float(cap) + fact[2 + i]
                meta[w][way, 0, 2 + i : 3 + i, 0:half] = (
                    fact[4 + 3 * i] + fact[5 + 3 * i] + fact[6 + 3 * i]
                )

    fetch.wait()
    block = min(tok, 16)
    for start in range(0, tok, block):
        span = slice(start, start + block)
        values = tokens[span, :].astype(F32)
        center = values - jnp.mean(values, axis=-1, keepdims=True)
        spread = jnp.mean(center * center, axis=-1, keepdims=True)
        normed[span, :] = (center * lax.rsqrt(spread + EPSILON) * gain_ref[...]).astype(BF16)

    def put_in_order(w):
        for way in range(2):
            ring[w][way, 0] = jnp.dot(
                sort[way, w * half : (w + 1) * half, :], normed[...], preferred_element_type=F32
            ).astype(BF16)

    put_in_order(0)

    pl.semaphore_wait(barrier, 3)

    def matches(w, way, k):
        slots = lax.broadcasted_iota(jnp.int32, (cap, half), 0).astype(F32) + first_code
        return meta[w][way, k, 0:1, 0:half] == slots, meta[w][way, k, 1:2, 0:half] == slots

    def onehot(w, way, k):
        first, second = matches(w, way, k)
        return jnp.where(first | second, 1.0, 0.0).astype(BF16)

    def pass_on(w, k):
        for way in range(2):
            offset = late(way, k)
            came = (k > 0) & goes(w, 0, count(k - 1, offset))
            pl.when(came)(lambda: meta_copy(w, way, k - 1).wait_recv())
            pl.when(goes(w, 0, count(k, offset)))(lambda: meta_copy(w, way, k).start())
        for p in range(pieces):
            for way in range(2):
                offset = late(way, k)
                came = (k > 0) & goes(w, p, count(k - 1, offset))
                pl.when(came)(lambda: ring_copy(w, way, k - 1, p).wait_recv())
                pl.when(goes(w, p, count(k, offset)))(lambda: ring_copy(w, way, k, p).start())

    def select(w, k):
        slot = lax.rem(k, SLOTS)
        pl.when(k >= SLOTS)(lambda: rows_copy(w, k - SLOTS).wait_send())
        for way in range(2):
            rows_in[w][slot, way * cap : (way + 1) * cap] = jnp.dot(
                onehot(w, way, k), ring[w][way, k], preferred_element_type=F32
            ).astype(BF16)
        rows_copy(w, k).start()

    def expert_rows(w, k):
        rows_copy(w, k).wait_recv()
        block_rows = rows_in[w][lax.rem(k, SLOTS)]
        gate_pre = jnp.dot(block_rows, gate[...], preferred_element_type=F32)
        up_pre = jnp.dot(block_rows, up[...], preferred_element_type=F32)
        gate_cut = jnp.minimum(gate_pre, clamp_limit)
        up_cut = jnp.clip(up_pre, -clamp_limit, clamp_limit)
        active[...] = (
            (up_cut + 1.0) * (gate_cut * jax.nn.sigmoid(gate_cut * sigmoid_slope))
        ).astype(BF16)
        slot = lax.rem(k, 2)
        pl.when(k >= 2)(lambda: part_copy(w, k - 2).wait_send())
        for start in range(0, width, hidden):
            span = slice(start, start + hidden)
            partial = jnp.dot(active[...], down[:, span], preferred_element_type=F32)
            own_part[w][slot, :, span] = partial[:pair]
            sent_part[w][slot, :, span] = partial[pair:].astype(BF16)
        part_copy(w, k).start()

    def weigh(w, k):
        part_copy(w, k).wait_recv()
        slot = lax.rem(k, 2)
        for way in range(2):
            first, second = matches(w, way, k)
            scale = jnp.sum(
                jnp.where(first, meta[w][way, k, 2:3, 0:half], 0.0)
                + jnp.where(second, meta[w][way, k, 3:4, 0:half], 0.0),
                axis=1,
                keepdims=True,
            )
            span = slice(way * cap, (way + 1) * cap)
            whole = own_part[w][slot, span] + part_in[w][k, span].astype(F32)
            part_in[w][k, span] = (whole * scale).astype(BF16)

    def spread_rows(w, way, k):
        return lax.dot_general(
            onehot(w, way, k),
            part_in[w][k, way * cap : (way + 1) * cap],
            (((0,), (0,)), ((), ())),
            preferred_element_type=F32,
        ).astype(BF16)

    def bring_back(w, k):
        for way in range(2):
            added[w][way] = spread_rows(w, way, k)
        for p in range(pieces):
            for way in range(2):
                offset = late(way, k)
                held = goes(w, p, count(k, offset))
                pl.when(held)(lambda: back_copy(w, way, k + 1, p).wait_recv())

                @pl.when(goes(w, p, count(k - 1, offset)))
                def _():
                    span = pl.ds(p * piece, piece)
                    before = jnp.where(held, back[w][way, k, span].astype(F32), 0.0)
                    back[w][way, k, span] = (before + added[w][way, span].astype(F32)).astype(BF16)
                    back_copy(w, way, k, p).start()

    def within(value, low, high):
        return (value >= low) & (value <= high)

    @pl.loop(0, max(s + 2 * r for s, r in zip(starts, radii)) + 3)
    def _(i):
        for w in range(WAVES):
            k = i - starts[w]
            pl.when(within(k, 0, radii[w]))(lambda: pass_on(w, k))
            home = 2 * radii[w] + 3 - k
            pl.when(within(home, 1, radii[w]))(lambda: bring_back(w, home))

        @pl.when(i == 1)
        def _():
            for load in loads:
                load.wait()
            for w in range(1, WAVES):
                put_in_order(w)

        for w in range(WAVES):
            k = i - starts[w]
            pl.when(within(k, 1, radii[w] + 1))(lambda: expert_rows(w, k - 1))
            pl.when(within(k, 0, radii[w]))(lambda: select(w, k))
            pl.when(within(k, 2, radii[w] + 2))(lambda: weigh(w, k - 2))

    total = None
    for w in range(WAVES):
        for p in range(pieces):
            for way in range(2):
                back_copy(w, way, 1, p).wait_recv()
        for way, part in ((0, spread_rows(w, 0, 0)), (0, back[w][0, 0]), (1, back[w][1, 0])):
            share = lax.dot_general(
                sort[way, w * half : (w + 1) * half, :],
                part,
                (((0,), (0,)), ((), ())),
                preferred_element_type=F32,
            )
            total = share if total is None else total + share
    out_ref[...] = total.astype(BF16)

    for w in range(WAVES):

        @pl.loop(0, radii[w] + 1)
        def _(k):
            pl.when(k > radii[w] - SLOTS)(lambda: rows_copy(w, k).wait_send())
            pl.when(k > radii[w] - 2)(lambda: part_copy(w, k).wait_send())
            for way in range(2):
                offset = late(way, k)
                rows = count(k, offset)
                pl.when(goes(w, 0, rows))(lambda: meta_copy(w, way, k).wait_send())
                for p in range(pieces):
                    pl.when(goes(w, p, rows))(lambda: ring_copy(w, way, k, p).wait_send())
                    sent = (k > 0) & goes(w, p, count(k - 1, offset))
                    pl.when(sent)(lambda: back_copy(w, way, k, p).wait_send())


def body(tokens, norm_gain, expert_ids, route_weight, gate_weight, up_weight, down_weight):
    devices = lax.axis_size("ep")
    tok, width = tokens.shape
    hidden = gate_weight.shape[2]
    experts, side, cap, half, radii, thin = plan(devices, tok, expert_ids.shape[1])
    piece = cap
    vmem = pl.BlockSpec(memory_space=pltpu.VMEM)
    hbm = pl.BlockSpec(memory_space=pl.ANY)
    dma = pltpu.SemaphoreType.DMA
    scratch = []
    for radius in radii:
        steps = radius + 1
        scratch += [
            pltpu.VMEM((2, steps, half, width), BF16),
            pltpu.VMEM((2, steps, half, width), BF16),
            pltpu.VMEM((2, steps, 8, tok), F32),
            pltpu.VMEM((SLOTS, 4 * cap, width), BF16),
            pltpu.VMEM((2, 2 * cap, width), F32),
            pltpu.VMEM((2, 2 * cap, width), BF16),
            pltpu.VMEM((steps, 2 * cap, width), BF16),
            pltpu.VMEM((2, half, width), BF16),
            dma((2, steps)),
            dma((2, steps)),
            dma((2, half // piece + 1, steps)),
            dma((2, half // piece + 1, steps)),
            dma((2, half // piece, steps)),
            dma((2, half // piece, steps)),
        ]
    scratch += [
        pltpu.VMEM((4 * cap, hidden), BF16),
        pltpu.VMEM((tok, width), BF16),
        pltpu.VMEM((tok, width), BF16),
        pltpu.VMEM((2, tok, tok), BF16),
        pltpu.VMEM((16, tok), F32),
        pltpu.VMEM((width, hidden), BF16),
        pltpu.VMEM((width, hidden), BF16),
        pltpu.VMEM((hidden, width), BF16),
        dma((4,)),
    ]
    return pl.pallas_call(
        functools.partial(kernel, devices, piece),
        out_shape=jax.ShapeDtypeStruct((tok, width), BF16),
        in_specs=[hbm] + [vmem] * 3 + [hbm] * 3,
        out_specs=vmem,
        scratch_shapes=scratch,
        compiler_params=pltpu.CompilerParams(
            collective_id=0, has_side_effects=True, vmem_limit_bytes=67043328
        ),
    )(
        tokens,
        norm_gain.reshape(1, width),
        expert_ids.T,
        route_weight.T,
        gate_weight,
        up_weight,
        down_weight,
    )


def solution(mesh):
    placed = (
        P(("grp", "ep"), None),
        P(),
        P(("grp", "ep"), None),
        P(("grp", "ep"), None),
        P("ep", None, None),
        P("ep", None, None),
        P("ep", None, None),
    )
    return jax.shard_map(
        body, mesh=mesh, in_specs=placed, out_specs=P(("grp", "ep"), None), check_vma=False
    )
```

```python
import functools

import jax
import jax.numpy as jnp
from jax import lax
from jax.experimental import pallas as pl
from jax.experimental.pallas import tpu as pltpu
from jax.sharding import PartitionSpec as P

SPLIT = 4
CORES = 2
WAVES = 2
LEAD = 11
SLOTS = 4
PARTS = 2

EPSILON = 1e-05
clamp_limit = 7.0
sigmoid_slope = 1.702
MESH = pl.DeviceIdType.MESH
F32 = jnp.float32
BF16 = jnp.bfloat16


def left_rows(tok, cap, side, k, offset):
    return min(tok, max(0, cap * (side - (k + offset) // 2)))


def plan(devices, tok, top_count):
    experts = devices // SPLIT
    side = experts // 2
    cap = min(tok, 2 * tok * top_count // experts)
    half = tok // WAVES
    radii, thin = [], []
    for w in range(WAVES):
        hops = range(1, devices // CORES + 1)
        radii.append(max(k for k in hops if left_rows(tok, cap, side, k - 1, 0) > w * half))
        full = (w + 1) * half
        thin.append(min(k for k in hops if left_rows(tok, cap, side, k - 1, 1) < full))
    return experts, side, cap, half, radii, thin


def kernel(
    devices,
    piece,
    tokens_hbm,
    gain_ref,
    ids_ref,
    weight_ref,
    gate_hbm,
    up_hbm,
    down_hbm,
    out_ref,
    *scratch,
):
    waves = [scratch[i * 15 : (i + 1) * 15] for i in range(WAVES)]
    active, tokens, normed, sort, rows, gate, up, down, load_sem = scratch[WAVES * 15 :]
    (
        ring,
        back,
        meta,
        rows_in,
        own_part,
        sent_part,
        part_in,
        added,
        row_sem,
        part_sem,
        ring_send,
        meta_send,
        ring_recv,
        back_send,
        back_recv,
    ) = zip(*waves)
    tok, width = tokens.shape
    hidden = gate.shape[1]
    experts, side, cap, half, radii, thin = plan(devices, tok, ids_ref.shape[0])
    pair = 2 * cap
    pieces = half // piece
    starts = [w * LEAD for w in range(WAVES)]

    me = lax.axis_index("ep")
    chip = lax.div(me, CORES)
    core = lax.rem(me, CORES)
    sibling = me + 1 - 2 * core
    upper = lax.rem(me + CORES, devices)
    lower = lax.rem(me + devices - CORES, devices)
    expert = lax.div(chip, SPLIT // CORES)
    first_code = (expert * cap).astype(F32)

    fetch = pltpu.make_async_copy(tokens_hbm, tokens, load_sem.at[0])
    fetch.start()
    loads = []
    for src, dst in ((gate_hbm, gate), (up_hbm, up), (down_hbm, down)):
        depth = dst.shape[0] // PARTS
        for j in range(PARTS):
            span = pl.ds(j * depth, depth)
            loads.append(
                pltpu.make_async_copy(src.at[0, span], dst.at[span], load_sem.at[len(loads) + 1])
            )

    def late(way, k):
        odd = lax.rem(chip + k, 2)
        return 1 - odd if way == 0 else odd

    def count(k, offset):
        left = cap * (side - lax.div(k + offset, 2))
        return jnp.minimum(tok, jnp.maximum(left, 0))

    def sent_rows(w, first):
        return [
            min(half, max(0, left_rows(tok, cap, side, k, (k + first) % 2) - w * half))
            for k in range(radii[w])
        ]

    def sent_slots(w, first):
        assert sum(sent_rows(w, first)) % half == 0
        return sum(sent_rows(w, first)) // half

    def sent_hops(w, first):
        return sum(r > 0 for r in sent_rows(w, first))

    def goes(w, p, rows):
        return rows > w * half + p * piece

    def remote(src, dst, send, recv, peer):
        return pltpu.make_async_remote_copy(
            src_ref=src,
            dst_ref=dst,
            send_sem=send,
            recv_sem=recv,
            device_id={"ep": peer},
            device_id_type=MESH,
        )

    def ring_copy(w, way, k, p):
        span = pl.ds(p * piece, piece)
        return remote(
            ring[w].at[way, k, span],
            ring[w].at[way, k + 1, span],
            ring_send[w].at[way],
            ring_recv[w].at[way, p, lax.rem(k + 1, SLOTS)],
            upper if way == 0 else lower,
        )

    def meta_copy(w, way, k):
        return remote(
            meta[w].at[way, k],
            meta[w].at[way, k + 1],
            meta_send[w].at[way],
            ring_recv[w].at[way, pieces, lax.rem(k + 1, SLOTS)],
            upper if way == 0 else lower,
        )

    def back_copy(w, way, k, p):
        span = pl.ds(p * piece, piece)
        return remote(
            back[w].at[way, k, span],
            back[w].at[way, k - 1, span],
            back_send[w].at[way],
            back_recv[w].at[way, p, lax.rem(k - 1, SLOTS)],
            lower if way == 0 else upper,
        )

    def rows_copy(w, k):
        slot = lax.rem(k, SLOTS)
        return remote(
            rows_in[w].at[slot, pl.ds(0, pair)],
            rows_in[w].at[slot, pl.ds(pair, pair)],
            row_sem[w].at[0, slot],
            row_sem[w].at[1, slot],
            sibling,
        )

    def part_copy(w, k):
        slot = lax.rem(k, SLOTS)
        return remote(
            sent_part[w].at[lax.rem(k, 2)],
            part_in[w].at[k],
            part_sem[w].at[0, slot],
            part_sem[w].at[1, slot],
            sibling,
        )

    for w in range(WAVES):

        @pl.loop(thin[w], radii[w] + 1)
        def _(k):
            for way in range(2):
                ring[w][way, k] = jnp.zeros((half, width), BF16)
                meta[w][way, k] = jnp.full(meta[w].shape[2:], -1.0, F32)

    barrier = pltpu.get_barrier_semaphore()
    for peer in (upper, lower, sibling):
        pl.semaphore_signal(barrier, inc=1, device_id={"ep": peer}, device_id_type=MESH)

    def reach(ids, way):
        offset = late(way, 0)
        steps = ids - expert if way == 0 else expert - ids
        steps = jnp.where(steps < 0, steps + experts, steps)
        inside = (steps >= 1 - offset) & (steps <= side - offset)
        return jnp.where(inside, 2 * steps + offset, 0).astype(F32)

    def across(left, right):
        return lax.dot_general(left, right, (((1,), (1,)), ((), ())), preferred_element_type=F32)

    row_index = lax.broadcasted_iota(jnp.int32, (tok, tok), 0)
    col_index = lax.broadcasted_iota(jnp.int32, (tok, tok), 1)
    earlier = row_index < col_index
    ids = [ids_ref[i : i + 1, :] for i in range(2)]
    id_row = [each.astype(F32) for each in ids]
    key_row = [jnp.maximum(reach(ids[0], way), reach(ids[1], way)) for way in range(2)]
    rows[...] = jnp.zeros_like(rows)
    for i, row in enumerate((*id_row, *key_row)):
        rows[i : i + 1, :] = row
    identity = jnp.where(row_index == col_index, 1.0, 0.0).astype(BF16)
    columns = across(identity, rows[...].astype(BF16))
    id_col = [columns[:, i : i + 1] for i in range(2)]
    for way in range(2):
        key_col = columns[:, 2 + way : 3 + way]
        behind = (key_col > key_row[way]) | ((key_col == key_row[way]) & earlier)
        rank = jnp.sum(jnp.where(behind, 1.0, 0.0), axis=0, keepdims=True).astype(jnp.int32)
        sort[way] = jnp.where(row_index == rank, 1.0, 0.0).astype(BF16)
    for i in range(2):
        same = ((id_col[0] == id_row[i]) | (id_col[1] == id_row[i])) & earlier
        rows[i : i + 1, :] = id_row[i]
        rows[2 + i : 3 + i, :] = jnp.sum(jnp.where(same, 1.0, 0.0), axis=0, keepdims=True)
        rest = weight_ref[i : i + 1, :]
        for j in range(3):
            high = rest.astype(BF16).astype(F32)
            rows[4 + 3 * i + j : 5 + 3 * i + j, :] = high
            rest = rest - high
    facts = rows[...].astype(BF16)
    for w in range(WAVES):
        for way in range(2):
            sorted_facts = across(facts, sort[way, w * half : (w + 1) * half, :])
            fact = [sorted_facts[i : i + 1] for i in range(10)]
            meta[w][way, 0] = jnp.full(meta[w].shape[2:], -1.0, F32)
            for i in range(2):
                meta[w][way, 0, i : i + 1, 0:half] = fact[i] * float(cap) + fact[2 + i]
                meta[w][way, 0, 2 + i : 3 + i, 0:half] = (
                    fact[4 + 3 * i] + fact[5 + 3 * i] + fact[6 + 3 * i]
                )

    fetch.wait()
    for load in loads:
        load.start()
    block = min(tok, 16)
    for start in range(0, tok, block):
        span = slice(start, start + block)
        values = tokens[span, :].astype(F32)
        center = values - jnp.mean(values, axis=-1, keepdims=True)
        spread = jnp.mean(center * center, axis=-1, keepdims=True)
        normed[span, :] = (center * lax.rsqrt(spread + EPSILON) * gain_ref[...]).astype(BF16)

    def put_in_order(w):
        for way in range(2):
            ring[w][way, 0] = jnp.dot(
                sort[way, w * half : (w + 1) * half, :], normed[...], preferred_element_type=F32
            ).astype(BF16)

    put_in_order(0)

    pl.semaphore_wait(barrier, 3)

    def matches(w, way, k):
        slots = lax.broadcasted_iota(jnp.int32, (cap, half), 0).astype(F32) + first_code
        return meta[w][way, k, 0:1, 0:half] == slots, meta[w][way, k, 1:2, 0:half] == slots

    def onehot(w, way, k):
        first, second = matches(w, way, k)
        return jnp.where(first | second, 1.0, 0.0).astype(BF16)

    def pass_on(w, k):
        for way in range(2):
            offset = late(way, k)
            came = (k > 0) & goes(w, 0, count(k - 1, offset))
            pl.when(came)(lambda: meta_copy(w, way, k - 1).wait_recv())
            pl.when(goes(w, 0, count(k, offset)))(lambda: meta_copy(w, way, k).start())
        for p in range(pieces):
            for way in range(2):
                offset = late(way, k)
                came = (k > 0) & goes(w, p, count(k - 1, offset))
                pl.when(came)(lambda: ring_copy(w, way, k - 1, p).wait_recv())
                pl.when(goes(w, p, count(k, offset)))(lambda: ring_copy(w, way, k, p).start())

    def select(w, k):
        slot = lax.rem(k, SLOTS)
        pl.when(k >= SLOTS)(lambda: rows_copy(w, k - SLOTS).wait_send())
        for way in range(2):
            rows_in[w][slot, way * cap : (way + 1) * cap] = jnp.dot(
                onehot(w, way, k), ring[w][way, k], preferred_element_type=F32
            ).astype(BF16)
        rows_copy(w, k).start()

    def expert_rows(w, k):
        rows_copy(w, k).wait_recv()
        block_rows = rows_in[w][lax.rem(k, SLOTS)]
        gate_pre = jnp.dot(block_rows, gate[...], preferred_element_type=F32)
        up_pre = jnp.dot(block_rows, up[...], preferred_element_type=F32)
        gate_cut = jnp.minimum(gate_pre, clamp_limit)
        up_cut = jnp.clip(up_pre, -clamp_limit, clamp_limit)
        active[...] = (
            (up_cut + 1.0) * (gate_cut * jax.nn.sigmoid(gate_cut * sigmoid_slope))
        ).astype(BF16)
        slot = lax.rem(k, 2)
        pl.when(k >= 2)(lambda: part_copy(w, k - 2).wait_send())
        for start in range(0, width, hidden):
            span = slice(start, start + hidden)
            partial = jnp.dot(active[...], down[:, span], preferred_element_type=F32)
            own_part[w][slot, :, span] = partial[:pair]
            sent_part[w][slot, :, span] = partial[pair:].astype(BF16)
        part_copy(w, k).start()

    def weigh(w, k):
        part_copy(w, k).wait_recv()
        slot = lax.rem(k, 2)
        for way in range(2):
            first, second = matches(w, way, k)
            scale = jnp.sum(
                jnp.where(first, meta[w][way, k, 2:3, 0:half], 0.0)
                + jnp.where(second, meta[w][way, k, 3:4, 0:half], 0.0),
                axis=1,
                keepdims=True,
            )
            span = slice(way * cap, (way + 1) * cap)
            whole = own_part[w][slot, span] + part_in[w][k, span].astype(F32)
            part_in[w][k, span] = (whole * scale).astype(BF16)

    def spread_rows(w, way, k):
        return lax.dot_general(
            onehot(w, way, k),
            part_in[w][k, way * cap : (way + 1) * cap],
            (((0,), (0,)), ((), ())),
            preferred_element_type=F32,
        ).astype(BF16)

    def bring_back(w, k):
        for way in range(2):
            added[w][way] = spread_rows(w, way, k)
        for p in range(pieces):
            for way in range(2):
                offset = late(way, k)
                held = goes(w, p, count(k, offset))
                pl.when(held)(lambda: back_copy(w, way, k + 1, p).wait_recv())

                @pl.when(goes(w, p, count(k - 1, offset)))
                def _():
                    span = pl.ds(p * piece, piece)
                    before = jnp.where(held, back[w][way, k, span].astype(F32), 0.0)
                    back[w][way, k, span] = (before + added[w][way, span].astype(F32)).astype(BF16)
                    back_copy(w, way, k, p).start()

    def within(value, low, high):
        return (value >= low) & (value <= high)

    @pl.loop(0, max(s + 2 * r for s, r in zip(starts, radii)) + 3)
    def _(i):
        for w in range(WAVES):
            k = i - starts[w]
            pl.when(within(k, 0, radii[w]))(lambda: pass_on(w, k))
            home = 2 * radii[w] + 3 - k
            pl.when(within(home, 1, radii[w]))(lambda: bring_back(w, home))

        @pl.when(i == 1)
        def _():
            for load in loads:
                load.wait()
            for w in range(1, WAVES):
                put_in_order(w)

        for w in range(WAVES):
            k = i - starts[w]
            pl.when(within(k, 1, radii[w] + 1))(lambda: expert_rows(w, k - 1))
            pl.when(within(k, 0, radii[w]))(lambda: select(w, k))
            pl.when(within(k, 2, radii[w] + 2))(lambda: weigh(w, k - 2))

    total = None
    for w in range(WAVES):
        for p in range(pieces):
            for way in range(2):
                back_copy(w, way, 1, p).wait_recv()
        for way, part in ((0, spread_rows(w, 0, 0)), (0, back[w][0, 0]), (1, back[w][1, 0])):
            share = lax.dot_general(
                sort[way, w * half : (w + 1) * half, :],
                part,
                (((0,), (0,)), ((), ())),
                preferred_element_type=F32,
            )
            total = share if total is None else total + share
    out_ref[...] = total.astype(BF16)

    def finish(w, way, first):
        peer = upper if way == 0 else lower
        for buf, send, recv, slots in (
            (ring[w], ring_send[w], ring_recv[w], sent_slots(w, first)),
            (meta[w], meta_send[w], ring_recv[w], sent_hops(w, first)),
            (back[w], back_send[w], back_recv[w], sent_slots(w, 1 - first)),
        ):
            span = buf.at[way, pl.ds(0, slots)]
            remote(span, span, send.at[way], recv.at[way, 0, 0], peer).wait_send()

    for w in range(WAVES):
        for k in range(radii[w] + 1 - SLOTS, radii[w] + 1):
            rows_copy(w, k).wait_send()
        for k in range(radii[w] - 1, radii[w] + 1):
            part_copy(w, k).wait_send()
        for way in range(2):
            for first in range(2):
                pl.when(late(way, 0) == first)(lambda: finish(w, way, first))


def body(tokens, norm_gain, expert_ids, route_weight, gate_weight, up_weight, down_weight):
    devices = lax.axis_size("ep")
    tok, width = tokens.shape
    hidden = gate_weight.shape[2]
    experts, side, cap, half, radii, thin = plan(devices, tok, expert_ids.shape[1])
    piece = cap
    vmem = pl.BlockSpec(memory_space=pltpu.VMEM)
    hbm = pl.BlockSpec(memory_space=pl.ANY)
    dma = pltpu.SemaphoreType.DMA
    scratch = []
    for radius in radii:
        steps = radius + 1
        scratch += [
            pltpu.VMEM((2, steps, half, width), BF16),
            pltpu.VMEM((2, steps, half, width), BF16),
            pltpu.VMEM((2, steps, 8, tok), F32),
            pltpu.VMEM((SLOTS, 4 * cap, width), BF16),
            pltpu.VMEM((2, 2 * cap, width), F32),
            pltpu.VMEM((2, 2 * cap, width), BF16),
            pltpu.VMEM((steps, 2 * cap, width), BF16),
            pltpu.VMEM((2, half, width), BF16),
            dma((2, SLOTS)),
            dma((2, SLOTS)),
            dma((2,)),
            dma((2,)),
            dma((2, half // piece + 1, SLOTS)),
            dma((2,)),
            dma((2, half // piece, SLOTS)),
        ]
    scratch += [
        pltpu.VMEM((4 * cap, hidden), BF16),
        pltpu.VMEM((tok, width), BF16),
        pltpu.VMEM((tok, width), BF16),
        pltpu.VMEM((2, tok, tok), BF16),
        pltpu.VMEM((16, tok), F32),
        pltpu.VMEM((width, hidden), BF16),
        pltpu.VMEM((width, hidden), BF16),
        pltpu.VMEM((hidden, width), BF16),
        dma((3 * PARTS + 1,)),
    ]
    return pl.pallas_call(
        functools.partial(kernel, devices, piece),
        out_shape=jax.ShapeDtypeStruct((tok, width), BF16),
        in_specs=[hbm] + [vmem] * 3 + [hbm] * 3,
        out_specs=vmem,
        scratch_shapes=scratch,
        compiler_params=pltpu.CompilerParams(
            collective_id=0, has_side_effects=True, vmem_limit_bytes=67043328
        ),
    )(
        tokens,
        norm_gain.reshape(1, width),
        expert_ids.T,
        route_weight.T,
        gate_weight,
        up_weight,
        down_weight,
    )


def solution(mesh):
    placed = (
        P(("grp", "ep"), None),
        P(),
        P(("grp", "ep"), None),
        P(("grp", "ep"), None),
        P("ep", None, None),
        P("ep", None, None),
        P("ep", None, None),
    )
    return jax.shard_map(
        body, mesh=mesh, in_specs=placed, out_specs=P(("grp", "ep"), None), check_vma=False
    )
```

```python
import functools

import jax
import jax.numpy as jnp
from jax import lax
from jax.experimental import pallas as pl
from jax.experimental.pallas import tpu as pltpu
from jax.sharding import PartitionSpec as P

SPLIT = 4
CORES = 2
WAVES = 2
LEAD = 11
SLOTS = 4
PARTS = 2

EPSILON = 1e-05
clamp_limit = 7.0
sigmoid_slope = 1.702
MESH = pl.DeviceIdType.MESH
F32 = jnp.float32
BF16 = jnp.bfloat16


def left_rows(tok, cap, side, k, offset):
    return min(tok, max(0, cap * (side - (k + offset) // 2)))


def plan(devices, tok, top_count):
    experts = devices // SPLIT
    side = experts // 2
    cap = min(tok, 2 * tok * top_count // experts)
    half = tok // WAVES
    radii, thin = [], []
    for w in range(WAVES):
        hops = range(1, devices // CORES + 1)
        radii.append(max(k for k in hops if left_rows(tok, cap, side, k - 1, 0) > w * half))
        full = (w + 1) * half
        thin.append(min(k for k in hops if left_rows(tok, cap, side, k - 1, 1) < full))
    return experts, side, cap, half, radii, thin


def kernel(
    devices,
    piece,
    tokens_hbm,
    gain_ref,
    ids_ref,
    weight_ref,
    gate_hbm,
    up_hbm,
    down_hbm,
    out_ref,
    *scratch,
):
    waves = [scratch[i * 15 : (i + 1) * 15] for i in range(WAVES)]
    active, tokens, normed, sort, rows, gate, up, down, load_sem = scratch[WAVES * 15 :]
    (
        ring,
        back,
        meta,
        rows_in,
        own_part,
        sent_part,
        part_in,
        added,
        row_sem,
        part_sem,
        ring_send,
        meta_send,
        ring_recv,
        back_send,
        back_recv,
    ) = zip(*waves)
    tok, width = tokens.shape
    hidden = gate.shape[1]
    experts, side, cap, half, radii, thin = plan(devices, tok, ids_ref.shape[0])
    pair = 2 * cap
    pieces = half // piece
    starts = [w * LEAD for w in range(WAVES)]

    me = lax.axis_index("ep")
    chip = lax.div(me, CORES)
    core = lax.rem(me, CORES)
    sibling = me + 1 - 2 * core
    upper = lax.rem(me + CORES, devices)
    lower = lax.rem(me + devices - CORES, devices)
    expert = lax.div(chip, SPLIT // CORES)
    first_code = (expert * cap).astype(F32)

    fetch = pltpu.make_async_copy(tokens_hbm, tokens, load_sem.at[0])
    fetch.start()
    loads = []
    for src, dst in ((gate_hbm, gate), (up_hbm, up), (down_hbm, down)):
        depth = dst.shape[0] // PARTS
        for j in range(PARTS):
            span = pl.ds(j * depth, depth)
            loads.append(
                pltpu.make_async_copy(src.at[0, span], dst.at[span], load_sem.at[len(loads) + 1])
            )

    def late(way, k):
        odd = lax.rem(chip + k, 2)
        return 1 - odd if way == 0 else odd

    def count(k, offset):
        left = cap * (side - lax.div(k + offset, 2))
        return jnp.minimum(tok, jnp.maximum(left, 0))

    def sent_rows(w, first):
        return [
            min(half, max(0, left_rows(tok, cap, side, k, (k + first) % 2) - w * half))
            for k in range(radii[w])
        ]

    def sent_slots(w, first):
        assert sum(sent_rows(w, first)) % half == 0
        return sum(sent_rows(w, first)) // half

    def sent_hops(w, first):
        return sum(r > 0 for r in sent_rows(w, first))

    def goes(w, p, rows):
        return rows > w * half + p * piece

    def remote(src, dst, send, recv, peer):
        return pltpu.make_async_remote_copy(
            src_ref=src,
            dst_ref=dst,
            send_sem=send,
            recv_sem=recv,
            device_id={"ep": peer},
            device_id_type=MESH,
        )

    def ring_copy(w, way, k, p):
        span = pl.ds(p * piece, piece)
        return remote(
            ring[w].at[way, k, span],
            ring[w].at[way, k + 1, span],
            ring_send[w].at[way],
            ring_recv[w].at[way, p, lax.rem(k + 1, SLOTS)],
            upper if way == 0 else lower,
        )

    def meta_copy(w, way, k):
        return remote(
            meta[w].at[way, k],
            meta[w].at[way, k + 1],
            meta_send[w].at[way],
            ring_recv[w].at[way, pieces, lax.rem(k + 1, SLOTS)],
            upper if way == 0 else lower,
        )

    def back_copy(w, way, k, p):
        span = pl.ds(p * piece, piece)
        return remote(
            back[w].at[way, k, span],
            back[w].at[way, k - 1, span],
            back_send[w].at[way],
            back_recv[w].at[way, p, lax.rem(k - 1, SLOTS)],
            lower if way == 0 else upper,
        )

    def rows_copy(w, k):
        slot = lax.rem(k, SLOTS)
        return remote(
            rows_in[w].at[slot, pl.ds(0, pair)],
            rows_in[w].at[slot, pl.ds(pair, pair)],
            row_sem[w].at[0, slot],
            row_sem[w].at[1, slot],
            sibling,
        )

    def part_copy(w, k):
        slot = lax.rem(k, SLOTS)
        return remote(
            sent_part[w].at[lax.rem(k, 2)],
            part_in[w].at[k],
            part_sem[w].at[0, slot],
            part_sem[w].at[1, slot],
            sibling,
        )

    for w in range(WAVES):

        @pl.loop(thin[w], radii[w] + 1)
        def _(k):
            for way in range(2):
                ring[w][way, k] = jnp.zeros((half, width), BF16)
                meta[w][way, k] = jnp.full(meta[w].shape[2:], -1.0, F32)

    barrier = pltpu.get_barrier_semaphore()
    for peer in (upper, lower, sibling):
        pl.semaphore_signal(barrier, inc=1, device_id={"ep": peer}, device_id_type=MESH)

    def reach(ids, way):
        offset = late(way, 0)
        steps = ids - expert if way == 0 else expert - ids
        steps = jnp.where(steps < 0, steps + experts, steps)
        inside = (steps >= 1 - offset) & (steps <= side - offset)
        return jnp.where(inside, 2 * steps + offset, 0).astype(F32)

    def across(left, right):
        return lax.dot_general(left, right, (((1,), (1,)), ((), ())), preferred_element_type=F32)

    row_index = lax.broadcasted_iota(jnp.int32, (tok, tok), 0)
    col_index = lax.broadcasted_iota(jnp.int32, (tok, tok), 1)
    earlier = row_index < col_index
    ids = [ids_ref[i : i + 1, :] for i in range(2)]
    id_row = [each.astype(F32) for each in ids]
    key_row = [jnp.maximum(reach(ids[0], way), reach(ids[1], way)) for way in range(2)]
    rows[...] = jnp.zeros_like(rows)
    for i, row in enumerate((*id_row, *key_row)):
        rows[i : i + 1, :] = row
    identity = jnp.where(row_index == col_index, 1.0, 0.0).astype(BF16)
    columns = across(identity, rows[...].astype(BF16))
    id_col = [columns[:, i : i + 1] for i in range(2)]
    for way in range(2):
        key_col = columns[:, 2 + way : 3 + way]
        behind = (key_col > key_row[way]) | ((key_col == key_row[way]) & earlier)
        rank = jnp.sum(jnp.where(behind, 1.0, 0.0), axis=0, keepdims=True).astype(jnp.int32)
        sort[way] = jnp.where(row_index == rank, 1.0, 0.0).astype(BF16)
    for i in range(2):
        same = ((id_col[0] == id_row[i]) | (id_col[1] == id_row[i])) & earlier
        rows[i : i + 1, :] = id_row[i]
        rows[2 + i : 3 + i, :] = jnp.sum(jnp.where(same, 1.0, 0.0), axis=0, keepdims=True)
        rest = weight_ref[i : i + 1, :]
        for j in range(3):
            high = rest.astype(BF16).astype(F32)
            rows[4 + 3 * i + j : 5 + 3 * i + j, :] = high
            rest = rest - high
    facts = rows[...].astype(BF16)
    for w in range(WAVES):
        for way in range(2):
            sorted_facts = across(facts, sort[way, w * half : (w + 1) * half, :])
            fact = [sorted_facts[i : i + 1] for i in range(10)]
            meta[w][way, 0] = jnp.full(meta[w].shape[2:], -1.0, F32)
            for i in range(2):
                meta[w][way, 0, i : i + 1, 0:half] = fact[i] * float(cap) + fact[2 + i]
                meta[w][way, 0, 2 + i : 3 + i, 0:half] = (
                    fact[4 + 3 * i] + fact[5 + 3 * i] + fact[6 + 3 * i]
                )

    fetch.wait()
    for load in loads:
        load.start()
    block = min(tok, 16)
    for start in range(0, tok, block):
        span = slice(start, start + block)
        values = tokens[span, :].astype(F32)
        center = values - jnp.mean(values, axis=-1, keepdims=True)
        spread = jnp.mean(center * center, axis=-1, keepdims=True)
        normed[span, :] = (center * lax.rsqrt(spread + EPSILON) * gain_ref[...]).astype(BF16)

    def put_in_order(w):
        for way in range(2):
            ring[w][way, 0] = jnp.dot(
                sort[way, w * half : (w + 1) * half, :], normed[...], preferred_element_type=F32
            ).astype(BF16)

    put_in_order(0)

    pl.semaphore_wait(barrier, 3)

    def matches(w, way, k):
        slots = lax.broadcasted_iota(jnp.int32, (cap, half), 0).astype(F32) + first_code
        return meta[w][way, k, 0:1, 0:half] == slots, meta[w][way, k, 1:2, 0:half] == slots

    def onehot(w, way, k):
        first, second = matches(w, way, k)
        return jnp.where(first | second, 1.0, 0.0).astype(BF16)

    def pass_on(w, k):
        for way in range(2):
            offset = late(way, k)
            came = (k > 0) & goes(w, 0, count(k - 1, offset))
            pl.when(came)(lambda: meta_copy(w, way, k - 1).wait_recv())
            pl.when(goes(w, 0, count(k, offset)))(lambda: meta_copy(w, way, k).start())
        for p in range(pieces):
            for way in range(2):
                offset = late(way, k)
                came = (k > 0) & goes(w, p, count(k - 1, offset))
                pl.when(came)(lambda: ring_copy(w, way, k - 1, p).wait_recv())
                pl.when(goes(w, p, count(k, offset)))(lambda: ring_copy(w, way, k, p).start())

    def select(w, k):
        slot = lax.rem(k, SLOTS)
        pl.when(k >= SLOTS)(lambda: rows_copy(w, k - SLOTS).wait_send())
        for way in range(2):
            rows_in[w][slot, way * cap : (way + 1) * cap] = jnp.dot(
                onehot(w, way, k), ring[w][way, k], preferred_element_type=F32
            ).astype(BF16)
        rows_copy(w, k).start()

    def expert_rows(w, k):
        rows_copy(w, k).wait_recv()
        block_rows = rows_in[w][lax.rem(k, SLOTS)]
        gate_pre = jnp.dot(block_rows, gate[...], preferred_element_type=F32)
        up_pre = jnp.dot(block_rows, up[...], preferred_element_type=F32)
        gate_cut = jnp.minimum(gate_pre, clamp_limit)
        up_cut = jnp.clip(up_pre, -clamp_limit, clamp_limit)
        active[...] = (
            (up_cut + 1.0) * (gate_cut * jax.nn.sigmoid(gate_cut * sigmoid_slope))
        ).astype(BF16)
        slot = lax.rem(k, 2)
        pl.when(k >= 2)(lambda: part_copy(w, k - 2).wait_send())
        for start in range(0, width, hidden):
            span = slice(start, start + hidden)
            partial = jnp.dot(active[...], down[:, span], preferred_element_type=F32)
            own_part[w][slot, :, span] = partial[:pair]
            sent_part[w][slot, :, span] = partial[pair:].astype(BF16)
        part_copy(w, k).start()

    def weigh(w, k):
        part_copy(w, k).wait_recv()
        slot = lax.rem(k, 2)
        for way in range(2):
            first, second = matches(w, way, k)
            scale = jnp.sum(
                jnp.where(first, meta[w][way, k, 2:3, 0:half], 0.0)
                + jnp.where(second, meta[w][way, k, 3:4, 0:half], 0.0),
                axis=1,
                keepdims=True,
            )
            span = slice(way * cap, (way + 1) * cap)
            whole = own_part[w][slot, span] + part_in[w][k, span].astype(F32)
            part_in[w][k, span] = (whole * scale).astype(BF16)

    def spread_rows(w, way, k):
        return lax.dot_general(
            onehot(w, way, k),
            part_in[w][k, way * cap : (way + 1) * cap],
            (((0,), (0,)), ((), ())),
            preferred_element_type=F32,
        ).astype(BF16)

    def bring_back(w, k):
        for way in range(2):
            added[w][way] = spread_rows(w, way, k)
        for p in range(pieces):
            for way in range(2):
                offset = late(way, k)
                held = goes(w, p, count(k, offset))
                pl.when(held)(lambda: back_copy(w, way, k + 1, p).wait_recv())

                @pl.when(goes(w, p, count(k - 1, offset)))
                def _():
                    span = pl.ds(p * piece, piece)
                    before = jnp.where(held, back[w][way, k, span].astype(F32), 0.0)
                    back[w][way, k, span] = (before + added[w][way, span].astype(F32)).astype(BF16)
                    back_copy(w, way, k, p).start()

    def within(value, low, high):
        return (value >= low) & (value <= high)

    @pl.loop(0, max(s + 2 * r for s, r in zip(starts, radii)) + 3)
    def _(i):
        for w in range(WAVES):
            k = i - starts[w]
            pl.when(within(k, 0, radii[w]))(lambda: pass_on(w, k))
            home = 2 * radii[w] + 3 - k
            pl.when(within(home, 1, radii[w]))(lambda: bring_back(w, home))

        @pl.when(i == 1)
        def _():
            for load in loads:
                load.wait()
            for w in range(1, WAVES):
                put_in_order(w)

        for w in range(WAVES):
            k = i - starts[w]
            pl.when(within(k, 1, radii[w] + 1))(lambda: expert_rows(w, k - 1))
            pl.when(within(k, 0, radii[w]))(lambda: select(w, k))
            pl.when(within(k, 2, radii[w] + 2))(lambda: weigh(w, k - 2))

    total = None
    for w in range(WAVES):
        for p in range(pieces):
            for way in range(2):
                back_copy(w, way, 1, p).wait_recv()
        for way, part in ((0, spread_rows(w, 0, 0)), (0, back[w][0, 0]), (1, back[w][1, 0])):
            share = lax.dot_general(
                sort[way, w * half : (w + 1) * half, :],
                part,
                (((0,), (0,)), ((), ())),
                preferred_element_type=F32,
            )
            total = share if total is None else total + share
    out_ref[...] = total.astype(BF16)

    def finish(w, way, first):
        peer = upper if way == 0 else lower
        for buf, send, recv, slots in (
            (ring[w], ring_send[w], ring_recv[w], sent_slots(w, first)),
            (meta[w], meta_send[w], ring_recv[w], sent_hops(w, first)),
            (back[w], back_send[w], back_recv[w], sent_slots(w, 1 - first)),
        ):
            span = buf.at[way, pl.ds(0, slots)]
            remote(span, span, send.at[way], recv.at[way, 0, 0], peer).wait_send()

    for w in range(WAVES):
        for k in range(radii[w] + 1 - SLOTS, radii[w] + 1):
            rows_copy(w, k).wait_send()
        for k in range(radii[w] - 1, radii[w] + 1):
            part_copy(w, k).wait_send()
        for way in range(2):
            for first in range(2):
                pl.when(late(way, 0) == first)(lambda: finish(w, way, first))


def body(tokens, norm_gain, expert_ids, route_weight, gate_weight, up_weight, down_weight):
    devices = lax.axis_size("ep")
    tok, width = tokens.shape
    hidden = gate_weight.shape[2]
    experts, side, cap, half, radii, thin = plan(devices, tok, expert_ids.shape[1])
    piece = cap // 2
    vmem = pl.BlockSpec(memory_space=pltpu.VMEM)
    hbm = pl.BlockSpec(memory_space=pl.ANY)
    dma = pltpu.SemaphoreType.DMA
    scratch = []
    for radius in radii:
        steps = radius + 1
        scratch += [
            pltpu.VMEM((2, steps, half, width), BF16),
            pltpu.VMEM((2, steps, half, width), BF16),
            pltpu.VMEM((2, steps, 4, tok), F32),
            pltpu.VMEM((SLOTS, 4 * cap, width), BF16),
            pltpu.VMEM((2, 2 * cap, width), F32),
            pltpu.VMEM((2, 2 * cap, width), BF16),
            pltpu.VMEM((steps, 2 * cap, width), BF16),
            pltpu.VMEM((2, half, width), BF16),
            dma((2, SLOTS)),
            dma((2, SLOTS)),
            dma((2,)),
            dma((2,)),
            dma((2, half // piece + 1, SLOTS)),
            dma((2,)),
            dma((2, half // piece, SLOTS)),
        ]
    scratch += [
        pltpu.VMEM((4 * cap, hidden), BF16),
        pltpu.VMEM((tok, width), BF16),
        pltpu.VMEM((tok, width), BF16),
        pltpu.VMEM((2, tok, tok), BF16),
        pltpu.VMEM((16, tok), F32),
        pltpu.VMEM((width, hidden), BF16),
        pltpu.VMEM((width, hidden), BF16),
        pltpu.VMEM((hidden, width), BF16),
        dma((3 * PARTS + 1,)),
    ]
    return pl.pallas_call(
        functools.partial(kernel, devices, piece),
        out_shape=jax.ShapeDtypeStruct((tok, width), BF16),
        in_specs=[hbm] + [vmem] * 3 + [hbm] * 3,
        out_specs=vmem,
        scratch_shapes=scratch,
        compiler_params=pltpu.CompilerParams(
            collective_id=0, has_side_effects=True, vmem_limit_bytes=67043328
        ),
    )(
        tokens,
        norm_gain.reshape(1, width),
        expert_ids.T,
        route_weight.T,
        gate_weight,
        up_weight,
        down_weight,
    )


def solution(mesh):
    placed = (
        P(("grp", "ep"), None),
        P(),
        P(("grp", "ep"), None),
        P(("grp", "ep"), None),
        P("ep", None, None),
        P("ep", None, None),
        P("ep", None, None),
    )
    return jax.shard_map(
        body, mesh=mesh, in_specs=placed, out_specs=P(("grp", "ep"), None), check_vma=False
    )
```

```python
import functools

import jax
import jax.numpy as jnp
from jax import lax
from jax.experimental import pallas as pl
from jax.experimental.pallas import tpu as pltpu
from jax.sharding import PartitionSpec as P

SPLIT = 4
CORES = 2
WAVES = 2
LEAD = 11
SLOTS = 4
PARTS = 2

EPSILON = 1e-05
clamp_limit = 7.0
sigmoid_slope = 1.702
MESH = pl.DeviceIdType.MESH
F32 = jnp.float32
BF16 = jnp.bfloat16


def left_rows(tok, cap, side, k, offset):
    return min(tok, max(0, cap * (side - (k + offset) // 2)))


def plan(devices, tok, top_count):
    experts = devices // SPLIT
    side = experts // 2
    cap = min(tok, 2 * tok * top_count // experts)
    half = tok // WAVES
    radii, thin = [], []
    for w in range(WAVES):
        hops = range(1, devices // CORES + 1)
        radii.append(max(k for k in hops if left_rows(tok, cap, side, k - 1, 0) > w * half))
        full = (w + 1) * half
        thin.append(min(k for k in hops if left_rows(tok, cap, side, k - 1, 1) < full))
    return experts, side, cap, half, radii, thin


def kernel(
    devices,
    piece,
    tokens_hbm,
    gain_ref,
    ids_ref,
    weight_ref,
    gate_hbm,
    up_hbm,
    down_hbm,
    out_ref,
    *scratch,
):
    waves = [scratch[i * 15 : (i + 1) * 15] for i in range(WAVES)]
    active, tokens, normed, sort, rows, gate, up, down, load_sem = scratch[WAVES * 15 :]
    (
        ring,
        back,
        meta,
        rows_in,
        own_part,
        sent_part,
        part_in,
        added,
        row_sem,
        part_sem,
        ring_send,
        meta_send,
        ring_recv,
        back_send,
        back_recv,
    ) = zip(*waves)
    tok, width = tokens.shape
    hidden = gate.shape[1]
    experts, side, cap, half, radii, thin = plan(devices, tok, ids_ref.shape[0])
    pair = 2 * cap
    pieces = half // piece
    starts = [w * LEAD for w in range(WAVES)]

    me = lax.axis_index("ep")
    chip = lax.div(me, CORES)
    core = lax.rem(me, CORES)
    sibling = me + 1 - 2 * core
    upper = lax.rem(me + CORES, devices)
    lower = lax.rem(me + devices - CORES, devices)
    expert = lax.div(chip, SPLIT // CORES)
    first_code = (expert * cap).astype(F32)

    fetch = pltpu.make_async_copy(tokens_hbm, tokens, load_sem.at[0])
    fetch.start()
    loads = []
    for src, dst in ((gate_hbm, gate), (up_hbm, up), (down_hbm, down)):
        depth = dst.shape[0] // PARTS
        for j in range(PARTS):
            span = pl.ds(j * depth, depth)
            loads.append(
                pltpu.make_async_copy(src.at[0, span], dst.at[span], load_sem.at[len(loads) + 1])
            )

    def late(way, k):
        odd = lax.rem(chip + k, 2)
        return 1 - odd if way == 0 else odd

    def count(k, offset):
        left = cap * (side - lax.div(k + offset, 2))
        return jnp.minimum(tok, jnp.maximum(left, 0))

    def sent_rows(w, first):
        return [
            min(half, max(0, left_rows(tok, cap, side, k, (k + first) % 2) - w * half))
            for k in range(radii[w])
        ]

    def sent_slots(w, first):
        assert sum(sent_rows(w, first)) % half == 0
        return sum(sent_rows(w, first)) // half

    def sent_hops(w, first):
        return sum(r > 0 for r in sent_rows(w, first))

    def goes(w, p, rows):
        return rows > w * half + p * piece

    def remote(src, dst, send, recv, peer):
        return pltpu.make_async_remote_copy(
            src_ref=src,
            dst_ref=dst,
            send_sem=send,
            recv_sem=recv,
            device_id={"ep": peer},
            device_id_type=MESH,
        )

    def ring_copy(w, way, k, p):
        span = pl.ds(p * piece, piece)
        return remote(
            ring[w].at[way, k, span],
            ring[w].at[way, k + 1, span],
            ring_send[w].at[way],
            ring_recv[w].at[way, p, lax.rem(k + 1, SLOTS)],
            upper if way == 0 else lower,
        )

    def meta_copy(w, way, k):
        return remote(
            meta[w].at[way, k],
            meta[w].at[way, k + 1],
            meta_send[w].at[way],
            ring_recv[w].at[way, pieces, lax.rem(k + 1, SLOTS)],
            upper if way == 0 else lower,
        )

    def back_copy(w, way, k, p):
        span = pl.ds(p * piece, piece)
        return remote(
            back[w].at[way, k, span],
            back[w].at[way, k - 1, span],
            back_send[w].at[way],
            back_recv[w].at[way, p, lax.rem(k - 1, SLOTS)],
            lower if way == 0 else upper,
        )

    def rows_copy(w, k):
        slot = lax.rem(k, SLOTS)
        return remote(
            rows_in[w].at[slot, pl.ds(0, pair)],
            rows_in[w].at[slot, pl.ds(pair, pair)],
            row_sem[w].at[0, slot],
            row_sem[w].at[1, slot],
            sibling,
        )

    def part_copy(w, k):
        slot = lax.rem(k, SLOTS)
        return remote(
            sent_part[w].at[lax.rem(k, 2)],
            part_in[w].at[k],
            part_sem[w].at[0, slot],
            part_sem[w].at[1, slot],
            sibling,
        )

    for w in range(WAVES):

        @pl.loop(thin[w], radii[w] + 1)
        def _(k):
            for way in range(2):
                ring[w][way, k] = jnp.zeros((half, width), BF16)
                meta[w][way, k] = jnp.full(meta[w].shape[2:], -1.0, F32)

    barrier = pltpu.get_barrier_semaphore()
    for peer in (upper, lower, sibling):
        pl.semaphore_signal(barrier, inc=1, device_id={"ep": peer}, device_id_type=MESH)

    def reach(ids, way):
        offset = late(way, 0)
        steps = ids - expert if way == 0 else expert - ids
        steps = jnp.where(steps < 0, steps + experts, steps)
        inside = (steps >= 1 - offset) & (steps <= side - offset)
        return jnp.where(inside, 2 * steps + offset, 0).astype(F32)

    def across(left, right):
        return lax.dot_general(left, right, (((1,), (1,)), ((), ())), preferred_element_type=F32)

    row_index = lax.broadcasted_iota(jnp.int32, (tok, tok), 0)
    col_index = lax.broadcasted_iota(jnp.int32, (tok, tok), 1)
    earlier = row_index < col_index
    ids = [ids_ref[i : i + 1, :] for i in range(2)]
    id_row = [each.astype(F32) for each in ids]
    key_row = [jnp.maximum(reach(ids[0], way), reach(ids[1], way)) for way in range(2)]
    rows[...] = jnp.zeros_like(rows)
    for i, row in enumerate((*id_row, *key_row)):
        rows[i : i + 1, :] = row
    identity = jnp.where(row_index == col_index, 1.0, 0.0).astype(BF16)
    columns = across(identity, rows[...].astype(BF16))
    id_col = [columns[:, i : i + 1] for i in range(2)]
    for way in range(2):
        key_col = columns[:, 2 + way : 3 + way]
        behind = (key_col > key_row[way]) | ((key_col == key_row[way]) & earlier)
        rank = jnp.sum(jnp.where(behind, 1.0, 0.0), axis=0, keepdims=True).astype(jnp.int32)
        sort[way] = jnp.where(row_index == rank, 1.0, 0.0).astype(BF16)
    for i in range(2):
        same = ((id_col[0] == id_row[i]) | (id_col[1] == id_row[i])) & earlier
        rows[i : i + 1, :] = id_row[i]
        rows[2 + i : 3 + i, :] = jnp.sum(jnp.where(same, 1.0, 0.0), axis=0, keepdims=True)
        rest = weight_ref[i : i + 1, :]
        for j in range(3):
            high = rest.astype(BF16).astype(F32)
            rows[4 + 3 * i + j : 5 + 3 * i + j, :] = high
            rest = rest - high
    facts = rows[...].astype(BF16)
    for w in range(WAVES):
        for way in range(2):
            sorted_facts = across(facts, sort[way, w * half : (w + 1) * half, :])
            fact = [sorted_facts[i : i + 1] for i in range(10)]
            meta[w][way, 0] = jnp.full(meta[w].shape[2:], -1.0, F32)
            for i in range(2):
                lanes = slice(i * half, (i + 1) * half)
                meta[w][way, 0, 0:1, lanes] = fact[i] * float(cap) + fact[2 + i]
                meta[w][way, 0, 1:2, lanes] = (
                    fact[4 + 3 * i] + fact[5 + 3 * i] + fact[6 + 3 * i]
                )

    fetch.wait()
    for load in loads:
        load.start()
    block = min(tok, 16)
    for start in range(0, tok, block):
        span = slice(start, start + block)
        values = tokens[span, :].astype(F32)
        center = values - jnp.mean(values, axis=-1, keepdims=True)
        spread = jnp.mean(center * center, axis=-1, keepdims=True)
        normed[span, :] = (center * lax.rsqrt(spread + EPSILON) * gain_ref[...]).astype(BF16)

    def put_in_order(w):
        for way in range(2):
            ring[w][way, 0] = jnp.dot(
                sort[way, w * half : (w + 1) * half, :], normed[...], preferred_element_type=F32
            ).astype(BF16)

    put_in_order(0)

    pl.semaphore_wait(barrier, 3)

    def matches(w, way, k):
        slots = lax.broadcasted_iota(jnp.int32, (cap, half), 0).astype(F32) + first_code
        code = meta[w][way, k, 0:1, :]
        return code[:, 0:half] == slots, code[:, half : 2 * half] == slots

    def onehot(w, way, k):
        first, second = matches(w, way, k)
        return jnp.where(first | second, 1.0, 0.0).astype(BF16)

    def pass_on(w, k):
        for way in range(2):
            offset = late(way, k)
            came = (k > 0) & goes(w, 0, count(k - 1, offset))
            pl.when(came)(lambda: meta_copy(w, way, k - 1).wait_recv())
            pl.when(goes(w, 0, count(k, offset)))(lambda: meta_copy(w, way, k).start())
        for p in range(pieces):
            for way in range(2):
                offset = late(way, k)
                came = (k > 0) & goes(w, p, count(k - 1, offset))
                pl.when(came)(lambda: ring_copy(w, way, k - 1, p).wait_recv())
                pl.when(goes(w, p, count(k, offset)))(lambda: ring_copy(w, way, k, p).start())

    def select(w, k):
        slot = lax.rem(k, SLOTS)
        pl.when(k >= SLOTS)(lambda: rows_copy(w, k - SLOTS).wait_send())
        for way in range(2):
            rows_in[w][slot, way * cap : (way + 1) * cap] = jnp.dot(
                onehot(w, way, k), ring[w][way, k], preferred_element_type=F32
            ).astype(BF16)
        rows_copy(w, k).start()

    def expert_rows(w, k):
        rows_copy(w, k).wait_recv()
        block_rows = rows_in[w][lax.rem(k, SLOTS)]
        gate_pre = jnp.dot(block_rows, gate[...], preferred_element_type=F32)
        up_pre = jnp.dot(block_rows, up[...], preferred_element_type=F32)
        gate_cut = jnp.minimum(gate_pre, clamp_limit)
        up_cut = jnp.clip(up_pre, -clamp_limit, clamp_limit)
        active[...] = (
            (up_cut + 1.0) * (gate_cut * jax.nn.sigmoid(gate_cut * sigmoid_slope))
        ).astype(BF16)
        slot = lax.rem(k, 2)
        pl.when(k >= 2)(lambda: part_copy(w, k - 2).wait_send())
        for start in range(0, width, hidden):
            span = slice(start, start + hidden)
            partial = jnp.dot(active[...], down[:, span], preferred_element_type=F32)
            own_part[w][slot, :, span] = partial[:pair]
            sent_part[w][slot, :, span] = partial[pair:].astype(BF16)
        part_copy(w, k).start()

    def weigh(w, k):
        part_copy(w, k).wait_recv()
        slot = lax.rem(k, 2)
        for way in range(2):
            first, second = matches(w, way, k)
            share = meta[w][way, k, 1:2, :]
            scale = jnp.sum(
                jnp.where(first, share[:, 0:half], 0.0)
                + jnp.where(second, share[:, half : 2 * half], 0.0),
                axis=1,
                keepdims=True,
            )
            span = slice(way * cap, (way + 1) * cap)
            whole = own_part[w][slot, span] + part_in[w][k, span].astype(F32)
            part_in[w][k, span] = (whole * scale).astype(BF16)

    def spread_rows(w, way, k):
        return lax.dot_general(
            onehot(w, way, k),
            part_in[w][k, way * cap : (way + 1) * cap],
            (((0,), (0,)), ((), ())),
            preferred_element_type=F32,
        ).astype(BF16)

    def bring_back(w, k):
        for way in range(2):
            added[w][way] = spread_rows(w, way, k)
        for p in range(pieces):
            for way in range(2):
                offset = late(way, k)
                held = goes(w, p, count(k, offset))
                pl.when(held)(lambda: back_copy(w, way, k + 1, p).wait_recv())

                @pl.when(goes(w, p, count(k - 1, offset)))
                def _():
                    span = pl.ds(p * piece, piece)
                    before = jnp.where(held, back[w][way, k, span].astype(F32), 0.0)
                    back[w][way, k, span] = (before + added[w][way, span].astype(F32)).astype(BF16)
                    back_copy(w, way, k, p).start()

    def within(value, low, high):
        return (value >= low) & (value <= high)

    @pl.loop(0, max(s + 2 * r for s, r in zip(starts, radii)) + 3)
    def _(i):
        for w in range(WAVES):
            k = i - starts[w]
            pl.when(within(k, 0, radii[w]))(lambda: pass_on(w, k))
            home = 2 * radii[w] + 3 - k
            pl.when(within(home, 1, radii[w]))(lambda: bring_back(w, home))

        @pl.when(i == 1)
        def _():
            for load in loads:
                load.wait()
            for w in range(1, WAVES):
                put_in_order(w)

        for w in range(WAVES):
            k = i - starts[w]
            pl.when(within(k, 1, radii[w] + 1))(lambda: expert_rows(w, k - 1))
            pl.when(within(k, 0, radii[w]))(lambda: select(w, k))
            pl.when(within(k, 2, radii[w] + 2))(lambda: weigh(w, k - 2))

    total = None
    for w in range(WAVES):
        for p in range(pieces):
            for way in range(2):
                back_copy(w, way, 1, p).wait_recv()
        for way, part in ((0, spread_rows(w, 0, 0)), (0, back[w][0, 0]), (1, back[w][1, 0])):
            share = lax.dot_general(
                sort[way, w * half : (w + 1) * half, :],
                part,
                (((0,), (0,)), ((), ())),
                preferred_element_type=F32,
            )
            total = share if total is None else total + share
    out_ref[...] = total

    def finish(w, way, first):
        peer = upper if way == 0 else lower
        for buf, send, recv, slots in (
            (ring[w], ring_send[w], ring_recv[w], sent_slots(w, first)),
            (meta[w], meta_send[w], ring_recv[w], sent_hops(w, first)),
            (back[w], back_send[w], back_recv[w], sent_slots(w, 1 - first)),
        ):
            span = buf.at[way, pl.ds(0, slots)]
            remote(span, span, send.at[way], recv.at[way, 0, 0], peer).wait_send()

    for w in range(WAVES):
        for k in range(radii[w] + 1 - SLOTS, radii[w] + 1):
            rows_copy(w, k).wait_send()
        for k in range(radii[w] - 1, radii[w] + 1):
            part_copy(w, k).wait_send()
        for way in range(2):
            for first in range(2):
                pl.when(late(way, 0) == first)(lambda: finish(w, way, first))


def body(tokens, norm_gain, expert_ids, route_weight, gate_weight, up_weight, down_weight):
    devices = lax.axis_size("ep")
    tok, width = tokens.shape
    hidden = gate_weight.shape[2]
    experts, side, cap, half, radii, thin = plan(devices, tok, expert_ids.shape[1])
    piece = cap // 2
    vmem = pl.BlockSpec(memory_space=pltpu.VMEM)
    hbm = pl.BlockSpec(memory_space=pl.ANY)
    dma = pltpu.SemaphoreType.DMA
    scratch = []
    for radius in radii:
        steps = radius + 1
        scratch += [
            pltpu.VMEM((2, steps, half, width), BF16),
            pltpu.VMEM((2, steps, half, width), BF16),
            pltpu.VMEM((2, steps, 2, tok), F32),
            pltpu.VMEM((SLOTS, 4 * cap, width), BF16),
            pltpu.VMEM((2, 2 * cap, width), F32),
            pltpu.VMEM((2, 2 * cap, width), BF16),
            pltpu.VMEM((steps, 2 * cap, width), BF16),
            pltpu.VMEM((2, half, width), BF16),
            dma((2, SLOTS)),
            dma((2, SLOTS)),
            dma((2,)),
            dma((2,)),
            dma((2, half // piece + 1, SLOTS)),
            dma((2,)),
            dma((2, half // piece, SLOTS)),
        ]
    scratch += [
        pltpu.VMEM((4 * cap, hidden), BF16),
        pltpu.VMEM((tok, width), BF16),
        pltpu.VMEM((tok, width), BF16),
        pltpu.VMEM((2, tok, tok), BF16),
        pltpu.VMEM((16, tok), F32),
        pltpu.VMEM((width, hidden), BF16),
        pltpu.VMEM((width, hidden), BF16),
        pltpu.VMEM((hidden, width), BF16),
        dma((3 * PARTS + 1,)),
    ]
    return pl.pallas_call(
        functools.partial(kernel, devices, piece),
        out_shape=jax.ShapeDtypeStruct((tok, width), F32),
        in_specs=[hbm] + [vmem] * 3 + [hbm] * 3,
        out_specs=vmem,
        scratch_shapes=scratch,
        compiler_params=pltpu.CompilerParams(
            collective_id=0, has_side_effects=True, vmem_limit_bytes=67043328
        ),
    )(
        tokens,
        norm_gain.reshape(1, width),
        expert_ids.T,
        route_weight.T,
        gate_weight,
        up_weight,
        down_weight,
    ).astype(BF16)


def solution(mesh):
    placed = (
        P(("grp", "ep"), None),
        P(),
        P(("grp", "ep"), None),
        P(("grp", "ep"), None),
        P("ep", None, None),
        P("ep", None, None),
        P("ep", None, None),
    )
    return jax.shard_map(
        body, mesh=mesh, in_specs=placed, out_specs=P(("grp", "ep"), None), check_vma=False
    )
```
